32 devices in a mesh: kv: 8 (over z, x), tp: 4 (over y, core).
Axes of the slice: x: 2, y: 2, z: 4, core: 2. Of those that a mesh axis runs over, the one named last changes fastest.
Arguments:
- tokens: bfloat16 [64, 2048], P(None, 'kv'), may hold values from -16 to 16
- norm_gain: float32 [2048], P('kv'), may hold values from 0.1 to 1.9
- query_weight: bfloat16 [2048, 2048], P('kv', 'tp'), may hold values from -0.125 to 0.125
- key_weight: bfloat16 [2048, 2048], P('kv', 'tp'), may hold values from -0.125 to 0.125
- value_weight: bfloat16 [2048, 2048], P('kv', 'tp'), may hold values from -0.125 to 0.125
- gate_weight: bfloat16 [2048, 2048], P('kv', 'tp'), may hold values from -0.125 to 0.125
- beta_weight: bfloat16 [2048, 16], replicated, may hold values from -0.125 to 0.125
- decay_weight: bfloat16 [2048, 16], replicated, may hold values from -0.5 to 0.5
- decay_rate: float32 [16], P('tp'), may hold values from 0.0005 to 0.1
- head_gain: float32 [128], replicated, may hold values from 0.1 to 1.9
- carried_state: float32 [64, 16, 128, 128], P('kv', 'tp'), may hold values from -4 to 4
- block_keys: bfloat16 [64, 16, 64, 128], P('kv', 'tp'), may hold values from -1 to 1, as said below
- block_values: bfloat16 [64, 16, 64, 128], P('kv', 'tp'), may hold values from -6 to 6
- block_beta: float32 [64, 16, 64], P('kv', 'tp'), may hold values from 0.1 to 0.9
- block_decay: float32 [64, 16, 64], P('kv', 'tp'), may hold values from -1.2 to 0
- live_count: int32 [64], P('kv'), may hold values from 1 to 64, 1638 in all
- out_weight: bfloat16 [2048, 2048], P('tp', 'kv'), may hold values from -0.125 to 0.125
- mlp_gain: float32 [2048], replicated, may hold values from 0.1 to 1.9
- up_weight: bfloat16 [2048, 8192], P('kv', 'tp'), may hold values from -0.125 to 0.125
- down_weight: bfloat16 [8192, 2048], P('tp', 'kv'), may hold values from -0.0625 to 0.0625
Outputs:
- mixed: bfloat16 [64, 2048], P(None, 'kv')
- new_state: float32 [64, 16, 128, 128], P('kv', 'tp')
The draws below stay inside these ranges and needn't reach their ends.
Inputs may be any that keep to these rules, and one draw needn't show every extreme that they name: `block_keys`: every key vector along the last dimension has unit length up to rounding.
All inputs are finite; a program needn't handle non-finite values. No bound on the sum of `live_count` on one device may be relied on, other than what follows from the above.
Results may differ from the reference program's by a relative error of at most 0.023.
Values may be sent and summed in bfloat16 or wider, within the bound.
No kernel may reach another device: no remote copies, remote signals or barrier semaphores. Data moves between devices by JAX's collectives and lax.ppermute only.
A program may use at most 64 MiB of HBM per device.

```python
import math
import jax
import jax.numpy as jnp
import numpy as np
from jax import lax

MODEL = 2048
HEADS = 16
HEAD_DIM = 128
MLP_UNITS = 8192
BLOCK_POSITIONS = 64
SEQ_DEV = 8
BATCH_TOTAL = 64
N_KV = 8
N_TP = 4


def head_rates(key):
    key_pick, key_fast, key_slow = jax.random.split(jax.random.fold_in(key, 11), 3)
    fast_heads = jax.random.randint(key_pick, (HEADS,), 0, 2) == 1
    fast_rate = jnp.exp(jax.random.uniform(key_fast, (HEADS,), jnp.float32, jnp.log(0.03), jnp.log(0.1)))
    slow_rate = jnp.exp(jax.random.uniform(key_slow, (HEADS,), jnp.float32, jnp.log(0.001), jnp.log(0.01)))
    return jnp.where(fast_heads, fast_rate, slow_rate)


def draw_decay_rate(key, part):
    return head_rates(key).astype(jnp.float32)


def draw_block_decay(key, part):
    decay_rates = head_rates(key)
    sequence_multiplier = jnp.exp(jax.random.uniform(jax.random.fold_in(key, 12), (BATCH_TOTAL, 1, 1), jnp.float32, jnp.log(0.5), jnp.log(2.0)))
    coarse_multiplier = jnp.exp(jax.random.uniform(jax.random.fold_in(key, 13), (BATCH_TOTAL, HEADS, BLOCK_POSITIONS), jnp.float32, jnp.log(0.3), jnp.log(2.0)))
    spike_selector = jax.random.randint(jax.random.fold_in(key, 14), (BATCH_TOTAL, 1, BLOCK_POSITIONS), 0, BLOCK_POSITIONS // 2) == 0
    spike_penalty = jnp.log(jax.random.uniform(jax.random.fold_in(key, 15), (BATCH_TOTAL, 1, BLOCK_POSITIONS), jnp.float32, 0.5, 0.8))
    decay_logarithm = -(decay_rates[None, :, None] * sequence_multiplier * coarse_multiplier) + jnp.where(spike_selector, spike_penalty, 0.0)
    return decay_logarithm.astype(jnp.float32)


def draw_block_keys(key, part):
    key_shared, key_noise = jax.random.split(jax.random.fold_in(key, 21))
    shared_shape = (BATCH_TOTAL, HEADS, 1, HEAD_DIM)
    noise_shape = (BATCH_TOTAL, HEADS, BLOCK_POSITIONS, HEAD_DIM)
    shared = jax.random.normal(key_shared, shared_shape, jnp.float32)
    noise = jax.random.normal(key_noise, noise_shape, jnp.float32)
    raw_keys = 0.6 * shared + 0.8 * noise
    lengths_sq = jnp.sum(raw_keys * raw_keys, axis=3, keepdims=True) + 1e-06
    return (raw_keys / jnp.sqrt(lengths_sq)).astype(jnp.bfloat16)


def draw_tokens(key, part):
    key_rough, key_vals = jax.random.split(key, 2)
    column_ramp = jnp.exp(jnp.log(4.0) * jnp.arange(MODEL, dtype=jnp.float32) / MODEL)
    rough_scale = jnp.exp(jax.random.uniform(key_rough, (MODEL,), jnp.float32, -0.5, 0.5))
    entries = jax.random.normal(key_vals, (BATCH_TOTAL, MODEL), jnp.float32)
    return jnp.clip(entries * column_ramp * rough_scale * 0.6, -16.0, 16.0).astype(jnp.bfloat16)


def block_scale(key, shape, shards, low, top_value):
    level, own = 1.0, jax.random.fold_in(key, 6)
    for dim, shards_of in shards:
        steps = jnp.exp(jax.random.uniform(jax.random.fold_in(own, dim), (shards_of,), jnp.float32, low / len(shards), top_value / len(shards)))
        level = level * jnp.repeat(steps, shape[dim] // shards_of).reshape([-1 if axis == dim else 1 for axis in range(len(shape))])
    return level


def split_up(count, total, reach, lean):
    portions = [(1 << 20) // math.isqrt(grade ** lean) + 1 for grade in range(2, count + 1)]
    rest, counts = total - reach - (count - 1), [1] * (count - 1)
    while rest > 0:
        free = [i for i in range(count - 1) if counts[i] < reach]
        whole, budget = sum([portions[i] for i in free]), rest
        for i in free:
            extra = min(reach - counts[i], max(1, budget * portions[i] // whole), rest)
            counts[i] = counts[i] + extra
            rest = rest - extra
    return np.array([reach] + counts)


def ragged(key, amount, total, most, lean):
    if amount == 2:
        one = jax.random.randint(key, (), max(1, total - most), min(most, total - 1) + 1)
        return jnp.stack([one, total - one])
    sizes = jnp.asarray(split_up(amount, total, most, lean), jnp.int32)
    couples = (amount - 1) // 2
    giver, receiver = sizes[1:1 + 2 * couples:2], sizes[2:2 + 2 * couples:2]
    margin = jnp.minimum(giver - 1, most - receiver)
    moved = jax.random.randint(jax.random.fold_in(key, 1), (couples,), 0, 1 << 20) % (margin + 1)
    sizes = sizes.at[1:1 + 2 * couples:2].set(giver - moved).at[2:2 + 2 * couples:2].set(receiver + moved)
    return sizes[jax.random.permutation(jax.random.fold_in(key, 2), amount)]


def scatter_about(own_key, shape, deviation, bound, pieces=(), held_as=jnp.bfloat16):
    drawn = deviation * jax.random.normal(own_key, shape, jnp.float32)
    if pieces:
        drawn = drawn * block_scale(own_key, shape, pieces, -0.22, 0.18)
    return jnp.clip(drawn, -bound, bound).astype(held_as)


def setup_inputs(seed: int = 0) -> dict:
    key_of = jax.random.split(jax.random.key(seed), 21)
    return {
        "tokens": draw_tokens(jax.random.fold_in(key_of[20], 71), 0),
        "norm_gain": jnp.clip(1.0 + 0.18 * jax.random.normal(key_of[1], (MODEL,), jnp.float32), 0.1, 1.9),
        "query_weight": scatter_about(key_of[2], (MODEL, HEADS * HEAD_DIM), MODEL ** -0.5, 0.125, ((0, 8), (1, 4))),
        "key_weight": scatter_about(key_of[3], (MODEL, HEADS * HEAD_DIM), MODEL ** -0.5, 0.125, ((0, 8), (1, 4))),
        "value_weight": scatter_about(key_of[4], (MODEL, HEADS * HEAD_DIM), MODEL ** -0.5, 0.125, ((0, 8), (1, 4))),
        "gate_weight": scatter_about(key_of[5], (MODEL, HEADS * HEAD_DIM), MODEL ** -0.5, 0.125, ((0, 8), (1, 4))),
        "beta_weight": scatter_about(key_of[6], (MODEL, HEADS), MODEL ** -0.5, 0.125),
        "decay_weight": scatter_about(key_of[7], (MODEL, HEADS), (MODEL // 16) ** -0.5, 0.5),
        "decay_rate": draw_decay_rate(jax.random.fold_in(key_of[20], 71), 0),
        "head_gain": jnp.clip(1.0 + 0.18 * jax.random.normal(key_of[9], (HEAD_DIM,), jnp.float32), 0.1, 1.9),
        "carried_state": scatter_about(key_of[10], (BATCH_TOTAL, HEADS, HEAD_DIM, HEAD_DIM), 0.3, 4.0, ((0, 8), (1, 4)), jnp.float32),
        "block_keys": draw_block_keys(jax.random.fold_in(key_of[20], 71), 0),
        "block_values": scatter_about(key_of[12], (BATCH_TOTAL, HEADS, BLOCK_POSITIONS, HEAD_DIM), 1.0, 6.0, ((0, 8), (1, 4))),
        "block_beta": jnp.clip(0.1 + 0.79999997 * jax.random.uniform(key_of[13], (BATCH_TOTAL, HEADS, BLOCK_POSITIONS), jnp.float32) ** block_scale(key_of[13], (BATCH_TOTAL, HEADS, BLOCK_POSITIONS), ((0, 8), (1, 4)), -0.2, 0.2), 0.1, 0.9),
        "block_decay": draw_block_decay(jax.random.fold_in(key_of[20], 71), 0),
        "live_count": ragged(key_of[15], BATCH_TOTAL, BATCH_TOTAL * BLOCK_POSITIONS * 2 // 5, BLOCK_POSITIONS, 2).astype(jnp.int32),
        "out_weight": scatter_about(key_of[16], (HEADS * HEAD_DIM, MODEL), (HEADS * HEAD_DIM) ** -0.5, 0.125, ((0, 4), (1, 8))),
        "mlp_gain": jnp.clip(1.0 + 0.18 * jax.random.normal(key_of[17], (MODEL,), jnp.float32), 0.1, 1.9),
        "up_weight": scatter_about(key_of[18], (MODEL, MLP_UNITS), MODEL ** -0.5, 0.125, ((0, 8), (1, 4))),
        "down_weight": scatter_about(key_of[19], (MLP_UNITS, MODEL), MLP_UNITS ** -0.5, 0.0625, ((0, 4), (1, 8))),
    }


EPS = 1e-06
PRECISE = lax.Precision.HIGHEST

def unit_inverse(strict_lower):
    slots_count = strict_lower.shape[-1]
    identity = jnp.eye(slots_count, dtype=strict_lower.dtype)
    powered = -strict_lower
    product_sum = identity + powered
    for repeat in range(slots_count.bit_length() - 2):
        powered = jnp.matmul(powered, powered, precision=PRECISE)
        product_sum = product_sum + jnp.matmul(product_sum, powered, precision=PRECISE)
    return product_sum

def delta_block(queries, key_new, value_new, beta_new, decay_new, keys, values, betas, decays, live_count, carried_state):
    slots_count = keys.shape[2]
    slot_ids = jnp.arange(slots_count, dtype=jnp.int32)
    newest = (live_count.astype(jnp.int32) - 1)[:, None, None]
    pending = slot_ids[None, None, :] < newest
    current = slot_ids[None, None, :] == newest
    keys_all = jnp.where(pending[..., None], keys, jnp.where(current[..., None], key_new[:, :, None, :], jnp.zeros_like(keys)))
    values_all = jnp.where(pending[..., None], values, jnp.where(current[..., None], value_new[:, :, None, :], jnp.zeros_like(values)))
    betas_all = jnp.where(pending, betas, jnp.where(current, beta_new[:, :, None], 0.0))
    decays_all = jnp.where(pending, decays, jnp.where(current, decay_new[:, :, None], 0.0))
    totals = jnp.cumsum(decays_all, axis=2)
    strict = slot_ids[:, None] > slot_ids[None, :]
    spread = jnp.where(strict, totals[..., :, None] - totals[..., None, :], 0.0)
    key_vals = keys_all.astype(jnp.float32)
    intersection = jnp.einsum('shid,shjd->shij', key_vals, key_vals, precision=PRECISE)
    strict_lower = jnp.where(strict, betas_all[..., :, None] * intersection * jnp.exp(spread), 0.0)
    inverse = unit_inverse(strict_lower)
    right_values = betas_all[..., None] * values_all.astype(jnp.float32)
    right_keys = (betas_all * jnp.exp(totals))[..., None] * key_vals
    solved_values = jnp.einsum('shij,shjv->shiv', inverse, right_values, precision=PRECISE)
    solved_keys = jnp.einsum('shij,shjk->shik', inverse, right_keys, precision=PRECISE)
    update = solved_values - jnp.einsum('shik,shkv->shiv', solved_keys, carried_state, precision=PRECISE)
    ending = totals[..., -1]
    faded_keys = key_vals * jnp.exp(ending[..., None] - totals)[..., None]
    new_state = jnp.exp(ending)[..., None, None] * carried_state + jnp.einsum('shik,shiv->shkv', faded_keys, update, precision=PRECISE)
    readout = jnp.einsum('shk,shkv->shv', queries, new_state, precision=PRECISE)
    return (readout, new_state)

def reference(tokens, norm_gain, query_weight, key_weight, value_weight, gate_weight, beta_weight, decay_weight, decay_rate, head_gain, carried_state, block_keys, block_values, block_beta, block_decay, live_count, out_weight, mlp_gain, up_weight, down_weight):
    token_vals = tokens.astype(jnp.float32)
    inverse_rms = lax.rsqrt(lax.optimization_barrier(jnp.mean(token_vals * token_vals, axis=1)) + EPS)[:, None]
    normed = (token_vals * norm_gain).astype(jnp.bfloat16)

    def project(weight):
        return jnp.dot(normed, weight, preferred_element_type=jnp.float32) * inverse_rms
    queries = project(query_weight).reshape(BATCH_TOTAL, HEADS, HEAD_DIM)
    key_raw = project(key_weight).reshape(BATCH_TOTAL, HEADS, HEAD_DIM)
    value_raw = project(value_weight).reshape(BATCH_TOTAL, HEADS, HEAD_DIM)
    gate_raw = project(gate_weight).reshape(BATCH_TOTAL, HEADS, HEAD_DIM)
    beta_new = jax.nn.sigmoid(project(beta_weight))
    decay_new = -decay_rate * jax.nn.softplus(project(decay_weight))
    key_new = (key_raw * lax.rsqrt(lax.optimization_barrier(jnp.sum(key_raw * key_raw, axis=2, keepdims=True)) + EPS)).astype(jnp.bfloat16)
    value_new = value_raw.astype(jnp.bfloat16)

    def grouped(array):
        return array.reshape((N_KV, SEQ_DEV) + array.shape[1:])
    grouped_args = tuple((grouped(item) for item in (queries, key_new, value_new, beta_new, decay_new, block_keys, block_values, block_beta, block_decay, live_count, carried_state)))
    readout, new_state = lax.map(lambda member: delta_block(*member), grouped_args)
    readout = readout.reshape(BATCH_TOTAL, HEADS, HEAD_DIM)
    new_state = new_state.reshape(BATCH_TOTAL, HEADS, HEAD_DIM, HEAD_DIM)
    scaled = readout * lax.rsqrt(lax.optimization_barrier(jnp.mean(readout * readout, axis=2, keepdims=True)) + EPS) * head_gain
    mixed_heads = (scaled * jax.nn.silu(gate_raw)).reshape(BATCH_TOTAL, HEADS * HEAD_DIM).astype(jnp.bfloat16)
    heads_dev = HEADS // N_TP
    blocks_in = mixed_heads.reshape(BATCH_TOTAL, N_TP, heads_dev * HEAD_DIM).astype(jnp.float32)
    blocks_weight = out_weight.reshape(N_TP, heads_dev * HEAD_DIM, MODEL).astype(jnp.float32)
    partial_value = jnp.einsum('btj,tjd->tbd', blocks_in, blocks_weight, precision=PRECISE)
    partial_value = lax.optimization_barrier(partial_value.astype(jnp.bfloat16)).astype(jnp.float32)
    attended = lax.optimization_barrier(jnp.sum(partial_value, axis=0))
    residual = lax.optimization_barrier((token_vals + attended).astype(jnp.bfloat16))
    resid_vals = residual.astype(jnp.float32)
    mlp_rms = lax.rsqrt(lax.optimization_barrier(jnp.mean(resid_vals * resid_vals, axis=1)) + EPS)[:, None]
    mlp_in = (resid_vals * mlp_gain).astype(jnp.bfloat16)
    pre_act = jnp.dot(mlp_in, up_weight, preferred_element_type=jnp.float32) * mlp_rms
    hidden = jnp.square(jax.nn.relu(pre_act)).astype(jnp.bfloat16)
    mixed = (resid_vals + jnp.dot(hidden, down_weight, preferred_element_type=jnp.float32)).astype(jnp.bfloat16)
    return (mixed, new_state)
```

```python
import jax
import jax.numpy as jnp
from jax import lax
from jax.sharding import PartitionSpec as P

MODEL = 2048


EPS = 1e-06
PRECISE = lax.Precision.HIGHEST


def unit_inverse(strict_lower):
    slots_count = strict_lower.shape[-1]
    identity = jnp.eye(slots_count, dtype=strict_lower.dtype)
    powered = -strict_lower
    product_sum = identity + powered
    for repeat in range(slots_count.bit_length() - 2):
        powered = jnp.matmul(powered, powered, precision=PRECISE)
        product_sum = product_sum + jnp.matmul(product_sum, powered, precision=PRECISE)
    return product_sum


def delta_block(
    queries,
    key_new,
    value_new,
    beta_new,
    decay_new,
    keys,
    values,
    betas,
    decays,
    live_count,
    carried_state,
):
    slots_count = keys.shape[2]
    slot_ids = jnp.arange(slots_count, dtype=jnp.int32)
    newest = (live_count - 1)[:, None, None]
    pending = slot_ids[None, None, :] < newest
    current = slot_ids[None, None, :] == newest
    keys_all = jnp.where(
        pending[..., None],
        keys,
        jnp.where(current[..., None], key_new[:, :, None, :], jnp.zeros_like(keys)),
    )
    values_all = jnp.where(
        pending[..., None],
        values,
        jnp.where(current[..., None], value_new[:, :, None, :], jnp.zeros_like(values)),
    )
    betas_all = jnp.where(pending, betas, jnp.where(current, beta_new[:, :, None], 0.0))
    decays_all = jnp.where(pending, decays, jnp.where(current, decay_new[:, :, None], 0.0))
    totals = jnp.cumsum(decays_all, axis=2)
    strict = slot_ids[:, None] > slot_ids[None, :]
    spread = jnp.where(strict, totals[..., :, None] - totals[..., None, :], 0.0)
    intersection = jnp.einsum(
        "shid,shjd->shij", keys_all, keys_all, preferred_element_type=jnp.float32
    )
    strict_lower = jnp.where(strict, betas_all[..., :, None] * intersection * jnp.exp(spread), 0.0)
    inverse = unit_inverse(strict_lower)
    key_vals = keys_all.astype(jnp.float32)
    right_values = betas_all[..., None] * values_all.astype(jnp.float32)
    right_keys = (betas_all * jnp.exp(totals))[..., None] * key_vals
    solved_values = jnp.einsum("shij,shjv->shiv", inverse, right_values, precision=PRECISE)
    solved_keys = jnp.einsum("shij,shjk->shik", inverse, right_keys, precision=PRECISE)
    update = solved_values - jnp.einsum(
        "shik,shkv->shiv", solved_keys, carried_state, precision=PRECISE
    )
    ending = totals[..., -1]
    faded_keys = key_vals * jnp.exp(ending[..., None] - totals)[..., None]
    new_state = jnp.exp(ending)[..., None, None] * carried_state + jnp.einsum(
        "shik,shiv->shkv", faded_keys, update, precision=PRECISE
    )
    readout = jnp.einsum("shk,shkv->shv", queries, new_state, precision=PRECISE)
    return (readout, new_state)


def scatter_sum(wide, extras):
    parts = lax.axis_size("kv")
    rows, width = wide.shape
    count = extras.shape[1]
    high = extras.astype(jnp.bfloat16)
    low = (extras - high.astype(jnp.float32)).astype(jnp.bfloat16)
    padding = jnp.zeros((rows, 128 - 2 * count), jnp.bfloat16)
    payload = jnp.concatenate([wide.astype(jnp.bfloat16), high, low, padding], axis=1)
    payload = payload.reshape(parts, rows // parts, width + 128)
    arrived = lax.all_to_all(payload, "kv", 0, 0, tiled=True).astype(jnp.float32)
    summed = jnp.sum(arrived, axis=0)
    tail = summed[:, width:]
    return summed[:, :width], tail[:, :count] + tail[:, count : 2 * count]


def gather_rows(mine):
    parts = lax.axis_size("kv")
    rows, width = mine.shape
    copies = jnp.broadcast_to(mine[None], (parts, rows, width))
    return lax.all_to_all(copies, "kv", 0, 0, tiled=True).reshape(parts * rows, width)


def sum_over_tp(part):
    count = lax.axis_size("tp")
    mine = part.astype(jnp.bfloat16)
    total = mine.astype(jnp.float32)
    for step in range(1, count):
        swaps = [(place, place ^ step) for place in range(count)]
        total = total + lax.ppermute(mine, "tp", swaps).astype(jnp.float32)
    return total


def body(
    tokens,
    norm_gain,
    query_weight,
    key_weight,
    value_weight,
    gate_weight,
    beta_weight,
    decay_weight,
    decay_rate,
    head_gain,
    carried_state,
    block_keys,
    block_values,
    block_beta,
    block_decay,
    live_count,
    out_weight,
    mlp_gain,
    up_weight,
    down_weight,
):
    kv_index = lax.axis_index("kv")
    tp_index = lax.axis_index("tp")
    columns = tokens.shape[1]
    seqs_here = carried_state.shape[0]
    heads_here = carried_state.shape[1]
    head_width = carried_state.shape[2]
    width = 4 * heads_here * head_width
    token_vals = tokens.astype(jnp.float32)
    squares = jnp.sum(token_vals * token_vals, axis=1)
    normed = (token_vals * norm_gain).astype(jnp.bfloat16)
    stacked = jnp.concatenate([query_weight, key_weight, value_weight, gate_weight], axis=1)
    beta_part = lax.dynamic_slice(
        beta_weight, (kv_index * columns, tp_index * heads_here), (columns, heads_here)
    )
    decay_part = lax.dynamic_slice(
        decay_weight, (kv_index * columns, tp_index * heads_here), (columns, heads_here)
    )
    small_weights = jnp.concatenate([beta_part, decay_part], axis=1)
    projected = jnp.dot(normed, stacked, preferred_element_type=jnp.float32)
    gating = jnp.dot(normed, small_weights, preferred_element_type=jnp.float32)
    extras = jnp.concatenate([squares[:, None], gating], axis=1)
    projected, extras = scatter_sum(projected, extras)
    inverse_rms = lax.rsqrt(extras[:, :1] / MODEL + EPS)
    gating = extras[:, 1:] * inverse_rms
    projected = (projected * inverse_rms).reshape(seqs_here, 4, heads_here, head_width)
    queries = projected[:, 0]
    key_raw = projected[:, 1]
    key_new = (key_raw * lax.rsqrt(jnp.sum(key_raw * key_raw, axis=2, keepdims=True) + EPS)).astype(
        jnp.bfloat16
    )
    value_new = projected[:, 2].astype(jnp.bfloat16)
    gate_raw = projected[:, 3]
    beta_new = jax.nn.sigmoid(gating[:, :heads_here])
    decay_new = -decay_rate * jax.nn.softplus(gating[:, heads_here:])
    readout, new_state = delta_block(
        queries,
        key_new,
        value_new,
        beta_new,
        decay_new,
        block_keys,
        block_values,
        block_beta,
        block_decay,
        live_count,
        carried_state,
    )
    scaled = (
        readout * lax.rsqrt(jnp.mean(readout * readout, axis=2, keepdims=True) + EPS) * head_gain
    )
    mixed_heads = (
        (scaled * jax.nn.silu(gate_raw))
        .reshape(seqs_here, heads_here * head_width)
        .astype(jnp.bfloat16)
    )
    attended = jnp.dot(gather_rows(mixed_heads), out_weight, preferred_element_type=jnp.float32)
    attended = sum_over_tp(attended)
    residual = lax.optimization_barrier((token_vals + attended).astype(jnp.bfloat16))
    resid_vals = residual.astype(jnp.float32)
    mlp_squares = jnp.sum(resid_vals * resid_vals, axis=1, keepdims=True)
    gain_part = lax.dynamic_slice_in_dim(mlp_gain, kv_index * columns, columns, 0)
    mlp_in = (resid_vals * gain_part).astype(jnp.bfloat16)
    pre_act = jnp.dot(mlp_in, up_weight, preferred_element_type=jnp.float32)
    pre_act, mlp_squares = scatter_sum(pre_act, mlp_squares)
    hidden = jnp.square(jax.nn.relu(pre_act * lax.rsqrt(mlp_squares / MODEL + EPS))).astype(
        jnp.bfloat16
    )
    output_part = jnp.dot(gather_rows(hidden), down_weight, preferred_element_type=jnp.float32)
    mixed = (resid_vals + sum_over_tp(output_part)).astype(jnp.bfloat16)
    return (mixed, new_state)


def solution(mesh):
    placed = (
        P(None, "kv"),
        P("kv"),
        P("kv", "tp"),
        P("kv", "tp"),
        P("kv", "tp"),
        P("kv", "tp"),
        P(),
        P(),
        P("tp"),
        P(),
        P("kv", "tp", None, None),
        P("kv", "tp", None, None),
        P("kv", "tp", None, None),
        P("kv", "tp", None),
        P("kv", "tp", None),
        P("kv"),
        P("tp", "kv"),
        P(),
        P("kv", "tp"),
        P("tp", "kv"),
    )
    return jax.shard_map(
        body,
        mesh=mesh,
        in_specs=placed,
        out_specs=(P(None, "kv"), P("kv", "tp", None, None)),
        check_vma=False,
    )
```

```python
import jax
import jax.numpy as jnp
from jax import lax
from jax.sharding import PartitionSpec as P

MODEL = 2048


EPS = 1e-06
def product(spec, left, right):
    return jnp.einsum(
        spec,
        left.astype(jnp.bfloat16),
        right.astype(jnp.bfloat16),
        preferred_element_type=jnp.float32,
    )


def unit_inverse(strict_lower):
    count = strict_lower.shape[-1]
    row = jnp.arange(count)[:, None]
    column = jnp.arange(count)[None, :]
    inverse = jnp.eye(count, dtype=jnp.float32) + jnp.zeros_like(strict_lower)
    size = 1
    while size < count:
        joins = (row // (2 * size) == column // (2 * size)) & (row // size != column // size)
        corner = jnp.where(joins, strict_lower, 0.0)
        if size == 1:
            inverse = inverse - corner
        else:
            middle = product("shij,shjk->shik", inverse, corner)
            inverse = inverse - product("shij,shjk->shik", middle, inverse)
        size *= 2
    return inverse


def earlier_state(keys, values, betas, decays, live_count, carried_state):
    count = keys.shape[2]
    slots = jnp.arange(count, dtype=jnp.int32)
    pending = (slots[None, :] < (live_count - 1)[:, None])[:, None, :]
    betas = jnp.where(pending, betas, 0.0)
    decays = jnp.where(pending, decays, 0.0)
    upto = (slots[:, None] <= slots[None, :]).astype(jnp.float32)
    totals = jnp.einsum("shi,ij->shj", decays, upto, precision=lax.Precision.HIGHEST)
    strict = slots[:, None] > slots[None, :]
    spread = jnp.where(strict, totals[..., :, None] - totals[..., None, :], 0.0)
    overlap = product("shid,shjd->shij", keys, keys)
    strict_lower = jnp.where(strict, betas[..., :, None] * overlap * jnp.exp(spread), 0.0)
    inverse = unit_inverse(strict_lower)
    recalled = product("shik,shkv->shiv", keys, carried_state)
    wanted = betas[..., None] * (values - jnp.exp(totals)[..., None] * recalled)
    update = product("shij,shjv->shiv", inverse, wanted)
    ending = totals[..., -1]
    faded = jnp.exp(ending[..., None] - totals)[..., None] * update
    return jnp.exp(ending)[..., None, None] * carried_state + product(
        "shik,shiv->shkv", keys, faded
    )


def newest_step(queries, key, value, beta, decay, state):
    key = key.astype(jnp.float32)[..., None]
    fade = jnp.exp(decay)[..., None]
    recalled = fade * jnp.sum(key * state, axis=2)
    update = beta[..., None] * (value.astype(jnp.float32) - recalled)
    answered = fade * jnp.sum(queries[..., None] * state, axis=2)
    readout = answered + jnp.sum(key[..., 0] * queries, axis=2, keepdims=True) * update
    new_state = fade[..., None] * state + key * update[:, :, None, :]
    return readout, new_state


def scatter_sum(wide, extras):
    parts = lax.axis_size("kv")
    rows, width = wide.shape
    count = extras.shape[1]
    high = extras.astype(jnp.bfloat16)
    low = (extras - high.astype(jnp.float32)).astype(jnp.bfloat16)
    padding = jnp.zeros((rows, 128 - 2 * count), jnp.bfloat16)
    payload = jnp.concatenate([wide.astype(jnp.bfloat16), high, low, padding], axis=1)
    payload = payload.reshape(parts, rows // parts, width + 128)
    arrived = lax.all_to_all(payload, "kv", 0, 0, tiled=True).astype(jnp.float32)
    summed = jnp.sum(arrived, axis=0)
    tail = summed[:, width:]
    return summed[:, :width], tail[:, :count] + tail[:, count : 2 * count]


def gather_rows(mine):
    parts = lax.axis_size("kv")
    rows, width = mine.shape
    copies = jnp.broadcast_to(mine[None], (parts, rows, width))
    return lax.all_to_all(copies, "kv", 0, 0, tiled=True).reshape(parts * rows, width)


def sum_over_tp(part):
    count = lax.axis_size("tp")
    mine = part.astype(jnp.bfloat16)
    total = mine.astype(jnp.float32)
    for step in range(1, count):
        swaps = [(place, place ^ step) for place in range(count)]
        total = total + lax.ppermute(mine, "tp", swaps).astype(jnp.float32)
    return total


def body(
    tokens,
    norm_gain,
    query_weight,
    key_weight,
    value_weight,
    gate_weight,
    beta_weight,
    decay_weight,
    decay_rate,
    head_gain,
    carried_state,
    block_keys,
    block_values,
    block_beta,
    block_decay,
    live_count,
    out_weight,
    mlp_gain,
    up_weight,
    down_weight,
):
    kv_index = lax.axis_index("kv")
    tp_index = lax.axis_index("tp")
    columns = tokens.shape[1]
    seqs_here = carried_state.shape[0]
    heads_here = carried_state.shape[1]
    head_width = carried_state.shape[2]
    width = 4 * heads_here * head_width
    token_vals = tokens.astype(jnp.float32)
    squares = jnp.sum(token_vals * token_vals, axis=1)
    normed = (token_vals * norm_gain).astype(jnp.bfloat16)
    stacked = jnp.concatenate([query_weight, key_weight, value_weight, gate_weight], axis=1)
    beta_part = lax.dynamic_slice(
        beta_weight, (kv_index * columns, tp_index * heads_here), (columns, heads_here)
    )
    decay_part = lax.dynamic_slice(
        decay_weight, (kv_index * columns, tp_index * heads_here), (columns, heads_here)
    )
    small_weights = jnp.concatenate([beta_part, decay_part], axis=1)
    projected = jnp.dot(normed, stacked, preferred_element_type=jnp.float32)
    gating = jnp.dot(normed, small_weights, preferred_element_type=jnp.float32)
    extras = jnp.concatenate([squares[:, None], gating], axis=1)
    projected, extras = scatter_sum(projected, extras)
    inverse_rms = lax.rsqrt(extras[:, :1] / MODEL + EPS)
    gating = extras[:, 1:] * inverse_rms
    projected = (projected * inverse_rms).reshape(seqs_here, 4, heads_here, head_width)
    queries = projected[:, 0]
    key_raw = projected[:, 1]
    key_new = (key_raw * lax.rsqrt(jnp.sum(key_raw * key_raw, axis=2, keepdims=True) + EPS)).astype(
        jnp.bfloat16
    )
    value_new = projected[:, 2].astype(jnp.bfloat16)
    gate_raw = projected[:, 3]
    beta_new = jax.nn.sigmoid(gating[:, :heads_here])
    decay_new = -decay_rate * jax.nn.softplus(gating[:, heads_here:])
    state = earlier_state(
        block_keys, block_values, block_beta, block_decay, live_count, carried_state
    )
    readout, new_state = newest_step(queries, key_new, value_new, beta_new, decay_new, state)
    scaled = (
        readout * lax.rsqrt(jnp.mean(readout * readout, axis=2, keepdims=True) + EPS) * head_gain
    )
    mixed_heads = (
        (scaled * jax.nn.silu(gate_raw))
        .reshape(seqs_here, heads_here * head_width)
        .astype(jnp.bfloat16)
    )
    attended = jnp.dot(gather_rows(mixed_heads), out_weight, preferred_element_type=jnp.float32)
    attended = sum_over_tp(attended)
    residual = lax.optimization_barrier((token_vals + attended).astype(jnp.bfloat16))
    resid_vals = residual.astype(jnp.float32)
    mlp_squares = jnp.sum(resid_vals * resid_vals, axis=1, keepdims=True)
    gain_part = lax.dynamic_slice_in_dim(mlp_gain, kv_index * columns, columns, 0)
    mlp_in = (resid_vals * gain_part).astype(jnp.bfloat16)
    pre_act = jnp.dot(mlp_in, up_weight, preferred_element_type=jnp.float32)
    pre_act, mlp_squares = scatter_sum(pre_act, mlp_squares)
    hidden = jnp.square(jax.nn.relu(pre_act * lax.rsqrt(mlp_squares / MODEL + EPS))).astype(
        jnp.bfloat16
    )
    output_part = jnp.dot(gather_rows(hidden), down_weight, preferred_element_type=jnp.float32)
    mixed = (resid_vals + sum_over_tp(output_part)).astype(jnp.bfloat16)
    return (mixed, new_state)


def solution(mesh):
    placed = (
        P(None, "kv"),
        P("kv"),
        P("kv", "tp"),
        P("kv", "tp"),
        P("kv", "tp"),
        P("kv", "tp"),
        P(),
        P(),
        P("tp"),
        P(),
        P("kv", "tp", None, None),
        P("kv", "tp", None, None),
        P("kv", "tp", None, None),
        P("kv", "tp", None),
        P("kv", "tp", None),
        P("kv"),
        P("tp", "kv"),
        P(),
        P("kv", "tp"),
        P("tp", "kv"),
    )
    return jax.shard_map(
        body,
        mesh=mesh,
        in_specs=placed,
        out_specs=(P(None, "kv"), P("kv", "tp", None, None)),
        check_vma=False,
    )
```

```python
import functools

import jax
import jax.numpy as jnp
from jax import lax
from jax.experimental import pallas as pl
from jax.experimental.pallas import tpu as pltpu
from jax.sharding import PartitionSpec as P

MODEL = 2048
EPS = 1e-06
LANES = 128
VMEM = pltpu.VMEM
SMEM = pltpu.SMEM


def in_vmem():
    return pl.BlockSpec(memory_space=VMEM)


def room(megabytes):
    return pltpu.CompilerParams(vmem_limit_bytes=megabytes << 20)


def held(value):
    return pltpu.with_memory_space_constraint(value, VMEM)


def afar(value):
    return pltpu.with_memory_space_constraint(value, pltpu.HBM)


def in_smem():
    return pl.BlockSpec(memory_space=SMEM)


def dot(left, right, contract=((1,), (0,)), precision=None):
    return lax.dot_general(
        left,
        right,
        (contract, ((), ())),
        precision=precision,
        preferred_element_type=jnp.float32,
    )


def halves(value):
    high = value.astype(jnp.bfloat16).astype(jnp.float32)
    return high, value - high


def project_kernel(
    at_ref,
    tokens_ref,
    gain_ref,
    beta_ref,
    decay_ref,
    *rest,
    count,
):
    weight_refs = rest[:count]
    out_ref = rest[count]
    buffers = rest[count + 1 : 2 * count + 1]
    semaphore = rest[2 * count + 1]
    copies = [
        pltpu.make_async_copy(weight_refs[i], buffers[i], semaphore.at[i]) for i in range(count)
    ]
    for copy in copies:
        copy.start()
    parts, rows, _ = out_ref.shape
    tokens = tokens_ref[...].astype(jnp.float32)
    batch = tokens.shape[0]
    normed = (tokens * gain_ref[...]).astype(jnp.bfloat16)
    squares = jnp.sum(tokens * tokens, axis=1, keepdims=True)
    heads = beta_ref.shape[0]
    small = jnp.concatenate(
        [
            beta_ref[...],
            decay_ref[...],
            jnp.zeros((LANES - 2 * heads, beta_ref.shape[1]), jnp.bfloat16),
        ],
        axis=0,
    )
    gating = dot(normed, small, ((1,), (1,)))
    lane = lax.broadcasted_iota(jnp.int32, (batch, LANES), 1)
    high, low = halves(gating)
    square_high, square_low = halves(squares)
    tile = high + pltpu.roll(low, 2 * heads, axis=1)
    tile = jnp.where(lane == 4 * heads, square_high, tile)
    tile = jnp.where(lane == 4 * heads + 1, square_low, tile)
    width = buffers[0].shape[1]
    out_ref[:, :, count * width :] = tile.reshape(parts, rows, LANES).astype(jnp.bfloat16)
    for i in range(count):
        copies[i].wait()
        made = dot(normed, buffers[i][...])
        out_ref[:, :, i * width : (i + 1) * width] = made.reshape(parts, rows, width).astype(
            jnp.bfloat16
        )


def project(kv_index, parts, tokens, norm_gain, weights, beta_weight, decay_weight):
    batch, columns = tokens.shape
    width = weights[0].shape[1]
    count = len(weights)
    betas, decays = beta_weight.T, decay_weight.T
    heads = betas.shape[0]
    where = kv_index
    if columns % LANES:
        betas = lax.dynamic_slice_in_dim(betas, kv_index * columns, columns, 1)
        decays = lax.dynamic_slice_in_dim(decays, kv_index * columns, columns, 1)
        where = jnp.zeros_like(kv_index)
    whole = lambda i, at: (0, 0)
    spec = pltpu.PrefetchScalarGridSpec(
        num_scalar_prefetch=1,
        grid=(1,),
        in_specs=[
            pl.BlockSpec((batch, columns), whole),
            pl.BlockSpec((1, columns), whole),
            pl.BlockSpec((heads, columns), lambda i, at: (0, at[0])),
            pl.BlockSpec((heads, columns), lambda i, at: (0, at[0])),
        ]
        + [pl.BlockSpec(memory_space=pl.ANY)] * count,
        out_specs=in_vmem(),
        scratch_shapes=[pltpu.VMEM((columns, width), jnp.bfloat16)] * count
        + [pltpu.SemaphoreType.DMA((count,))],
    )
    return pl.pallas_call(
        functools.partial(project_kernel, count=count),
        grid_spec=spec,
        out_shape=VMEM((parts, batch // parts, count * width + LANES), jnp.bfloat16),
        compiler_params=room(4),
        name="project",
    )(
        where.reshape(1),
        afar(tokens),
        afar(norm_gain.reshape(1, columns)),
        afar(betas),
        afar(decays),
        *[afar(weight) for weight in weights],
    )


def block_kernel(
    live_ref,
    keys_ref,
    values_ref,
    betas_ref,
    decays_ref,
    far_state_ref,
    out_ref,
    state_ref,
    semaphore,
    *,
    group,
):
    pairs, slots, _ = keys_ref.shape
    fetch = pltpu.make_async_copy(far_state_ref, state_ref, semaphore)
    fetch.start()
    row = lax.broadcasted_iota(jnp.int32, (slots, slots), 0)
    column = lax.broadcasted_iota(jnp.int32, (slots, slots), 1)
    strict = row > column
    pending = lax.broadcasted_iota(jnp.int32, (pairs, slots), 1) < live_ref[...] - 1
    betas = jnp.where(pending, betas_ref[...], 0.0)
    decays = jnp.where(pending, decays_ref[...], 0.0)
    upto = (row <= column).astype(jnp.float32)
    totals = dot(decays, upto, precision=lax.Precision.HIGHEST)
    columns = jnp.concatenate([totals, betas], axis=0).T
    total_columns = columns[:, :pairs]
    beta_columns = columns[:, pairs:]
    ending = total_columns[slots - 1 : slots, :]
    grown = jnp.exp(total_columns)
    faded = jnp.exp(ending - total_columns)
    whole_fade = jnp.exp(totals[:, slots - 1 : slots])
    identity = (row == column).astype(jnp.float32)
    sizes = []
    size = 1
    while size < slots:
        sizes.append(size)
        size *= 2
    joins = [(row // (2 * s) == column // (2 * s)) & (row // s != column // s) for s in sizes]
    for first in range(0, pairs, group):
        members = range(first, min(first + group, pairs))
        lower = {}
        inverse = {}
        for p in members:
            keys = keys_ref[p]
            overlap = dot(keys, keys, ((1,), (1,)))
            spread = total_columns[:, p : p + 1] - totals[p : p + 1, :]
            weight = jnp.exp(jnp.where(strict, spread, 0.0))
            lower[p] = jnp.where(strict, beta_columns[:, p : p + 1] * overlap * weight, 0.0)
            inverse[p] = identity - jnp.where(joins[0], lower[p], 0.0)
        for level in range(1, len(sizes)):
            short = {p: inverse[p].astype(jnp.bfloat16) for p in members}
            middle = {
                p: dot(short[p], jnp.where(joins[level], lower[p], 0.0).astype(jnp.bfloat16))
                for p in members
            }
            for p in members:
                inverse[p] = inverse[p] - dot(middle[p].astype(jnp.bfloat16), short[p])
        if first == 0:
            fetch.wait()
        for p in members:
            keys = keys_ref[p]
            state = state_ref[p]
            recalled = dot(keys, state.astype(jnp.bfloat16))
            wanted = beta_columns[:, p : p + 1] * (
                values_ref[p].astype(jnp.float32) - grown[:, p : p + 1] * recalled
            )
            update = dot(inverse[p].astype(jnp.bfloat16), wanted.astype(jnp.bfloat16))
            update = (faded[:, p : p + 1] * update).astype(jnp.bfloat16)
            out_ref[p] = whole_fade[p : p + 1, :] * state + dot(keys, update, ((0,), (0,)))


def block_state(live_count, keys, values, betas, decays, state, group=16):
    seqs, heads, slots, width = keys.shape
    pairs = seqs * heads
    live = jnp.repeat(live_count, heads).reshape(pairs, 1)
    return pl.pallas_call(
        functools.partial(block_kernel, group=group),
        in_specs=[in_vmem()] * 5 + [pl.BlockSpec(memory_space=pl.ANY)],
        out_specs=in_vmem(),
        scratch_shapes=[VMEM((pairs, width, width), jnp.float32), pltpu.SemaphoreType.DMA],
        out_shape=VMEM((pairs, width, width), jnp.float32),
        cost_estimate=pl.CostEstimate(
            flops=60_000_000, bytes_accessed=5_000_000, transcendentals=0
        ),
        compiler_params=room(24),
        name="block_state",
    )(
        held(live),
        held(keys.reshape(pairs, slots, width)),
        held(values.reshape(pairs, slots, width)),
        held(betas.reshape(pairs, slots)),
        held(decays.reshape(pairs, slots)),
        afar(state.reshape(pairs, width, width)),
    )


def newest_kernel(
    at_ref,
    rate_ref,
    arrived_ref,
    state_ref,
    gain_ref,
    mixed_ref,
    update_ref,
    columns_ref,
    fade_ref,
    recalled_ref,
    answered_ref,
    *,
    heads,
    total_heads,
):
    seqs = arrived_ref.shape[1]
    width = state_ref.shape[1]
    summed = jnp.sum(arrived_ref[...].astype(jnp.float32), axis=0)
    tail = summed[:, 4 * heads * width :]
    lane = lax.broadcasted_iota(jnp.int32, (seqs, LANES), 1)
    is_square = (lane == 4 * total_heads) | (lane == 4 * total_heads + 1)
    squares = jnp.sum(jnp.where(is_square, tail, 0.0), axis=1, keepdims=True)
    scale = lax.rsqrt(squares / MODEL + EPS)
    gating = (tail + pltpu.roll(tail, LANES - 2 * total_heads, axis=1)) * scale
    first = at_ref[0] * heads
    part = lambda i, h: summed[:, (i * heads + h) * width : (i * heads + h + 1) * width] * scale
    queries = [part(0, h) for h in range(heads)]
    keys = []
    for h in range(heads):
        raw = part(1, h)
        keys.append(raw * lax.rsqrt(jnp.sum(raw * raw, axis=1, keepdims=True) + EPS))
    keys = [key.astype(jnp.bfloat16).astype(jnp.float32) for key in keys]
    columns = jnp.concatenate(keys + queries, axis=0).T
    columns_ref[...] = columns
    count = heads * seqs
    for h in range(heads):
        for s in range(seqs):
            state = state_ref[s * heads + h]
            j = h * seqs + s
            key_column = columns[:, j : j + 1]
            query_column = columns[:, count + j : count + j + 1]
            recalled_ref[j : j + 1, :] = jnp.sum(key_column * state, axis=0, keepdims=True)
            answered_ref[j : j + 1, :] = jnp.sum(query_column * state, axis=0, keepdims=True)
    for h in range(heads):
        pick = lambda at: jnp.sum(jnp.where(lane == at, gating, 0.0), axis=1, keepdims=True)
        beta = jax.nn.sigmoid(pick(first + h))
        raw = pick(total_heads + first + h)
        softplus = jnp.maximum(raw, 0.0) + jnp.log1p(jnp.exp(-jnp.abs(raw)))
        fade = jnp.exp(-rate_ref[h] * softplus)
        rows = slice(h * seqs, (h + 1) * seqs)
        value = part(2, h).astype(jnp.bfloat16).astype(jnp.float32)
        update = beta * (value - fade * recalled_ref[rows, :])
        agreement = jnp.sum(keys[h] * queries[h], axis=1, keepdims=True)
        readout = fade * answered_ref[rows, :] + agreement * update
        update_ref[rows, :] = update
        fade_ref[rows, :] = jnp.broadcast_to(fade, (seqs, width))
        gate = part(3, h)
        power = jnp.mean(readout * readout, axis=1, keepdims=True)
        mixed = readout * lax.rsqrt(power + EPS) * gain_ref[...] * (gate * jax.nn.sigmoid(gate))
        shape = (mixed_ref.shape[0], seqs, width)
        mixed_ref[:, :, h * width : (h + 1) * width] = jnp.broadcast_to(mixed[None], shape).astype(
            jnp.bfloat16
        )


def newest(tp_index, decay_rate, arrived, state, head_gain, heads, total_heads):
    parts, seqs, _ = arrived.shape
    width = state.shape[1]
    count = heads * seqs
    return pl.pallas_call(
        functools.partial(newest_kernel, heads=heads, total_heads=total_heads),
        in_specs=[in_smem(), in_smem(), in_vmem(), in_vmem(), in_vmem()],
        out_specs=[in_vmem()] * 4,
        out_shape=[
            VMEM((parts, seqs, heads * width), jnp.bfloat16),
            VMEM((count, width), jnp.float32),
            VMEM((width, 2 * count), jnp.float32),
            VMEM((count, width), jnp.float32),
        ],
        scratch_shapes=[pltpu.VMEM((count, width), jnp.float32)] * 2,
        compiler_params=room(4),
        name="newest",
    )(
        tp_index.reshape(1),
        decay_rate,
        held(arrived),
        held(state),
        held(head_gain.reshape(1, width)),
    )


def refresh_kernel(state_ref, update_ref, columns_ref, fade_ref, out_ref, made_ref, semaphore):
    pairs = state_ref.shape[0]
    seqs = made_ref.shape[0]
    heads = pairs // seqs
    columns = columns_ref[...]
    copies = []
    for s in range(seqs):
        for h in range(heads):
            j = h * seqs + s
            made_ref[s, h] = (
                fade_ref[j : j + 1, :] * state_ref[s * heads + h]
                + columns[:, j : j + 1] * update_ref[j : j + 1, :]
            )
        copies.append(pltpu.make_async_copy(made_ref.at[s], out_ref.at[s], semaphore.at[s]))
        copies[-1].start()
    for copy in copies:
        copy.wait()


def refresh(state, update, columns, fade, seqs):
    pairs, width, _ = state.shape
    shape = (seqs, pairs // seqs, width, width)
    return pl.pallas_call(
        refresh_kernel,
        in_specs=[in_vmem()] * 4,
        out_specs=pl.BlockSpec(memory_space=pl.ANY),
        out_shape=jax.ShapeDtypeStruct(shape, jnp.float32),
        scratch_shapes=[pltpu.VMEM(shape, jnp.float32), pltpu.SemaphoreType.DMA((seqs,))],
        cost_estimate=pl.CostEstimate(
            flops=10_000_000, bytes_accessed=4_000_000, transcendentals=0
        ),
        compiler_params=room(8),
        name="refresh",
    )(held(state), held(update), held(columns), held(fade))


def widen_kernel(residual_ref, scaled_ref, weight_ref, out_ref):
    parts, rows, _ = out_ref.shape
    value = residual_ref[...].astype(jnp.float32)
    batch = value.shape[0]
    high, low = halves(jnp.sum(value * value, axis=1, keepdims=True))
    lane = lax.broadcasted_iota(jnp.int32, (batch, LANES), 1)
    tile = jnp.where(lane == 0, high, jnp.where(lane == 1, low, 0.0))
    units = weight_ref.shape[1]
    out_ref[:, :, units:] = tile.reshape(parts, rows, LANES).astype(jnp.bfloat16)
    made = dot(scaled_ref[...], weight_ref[...])
    out_ref[:, :, :units] = made.reshape(parts, rows, units).astype(jnp.bfloat16)


def widen(parts, residual, scaled, up_weight):
    batch = residual.shape[0]
    units = up_weight.shape[1]
    return pl.pallas_call(
        widen_kernel,
        in_specs=[in_vmem()] * 3,
        out_specs=in_vmem(),
        out_shape=VMEM((parts, batch // parts, units + LANES), jnp.bfloat16),
        compiler_params=room(6),
        name="widen",
    )(held(residual), held(scaled), held(up_weight))


def activate_kernel(arrived_ref, out_ref):
    units = out_ref.shape[2]
    summed = jnp.sum(arrived_ref[...].astype(jnp.float32), axis=0)
    tail = summed[:, units:]
    lane = lax.broadcasted_iota(jnp.int32, tail.shape, 1)
    squares = jnp.sum(jnp.where(lane < 2, tail, 0.0), axis=1, keepdims=True)
    scale = lax.rsqrt(squares / MODEL + EPS)
    hidden = jnp.square(jnp.maximum(summed[:, :units] * scale, 0.0))
    out_ref[...] = jnp.broadcast_to(hidden[None], out_ref.shape).astype(jnp.bfloat16)


def activate(arrived):
    parts, seqs, wide = arrived.shape
    return pl.pallas_call(
        activate_kernel,
        in_specs=[in_vmem()],
        out_specs=in_vmem(),
        out_shape=VMEM((parts, seqs, wide - LANES), jnp.bfloat16),
        compiler_params=room(4),
        name="activate",
    )(held(arrived))


def narrow_kernel(rows_ref, weight_ref, out_ref):
    rows = rows_ref[...]
    rows = rows.reshape(rows.shape[0] * rows.shape[1], rows.shape[2])
    out_ref[...] = dot(rows, weight_ref[...]).astype(jnp.bfloat16)


def narrow(rows, weight, name):
    return pl.pallas_call(
        narrow_kernel,
        in_specs=[in_vmem()] * 2,
        out_specs=in_vmem(),
        out_shape=VMEM((rows.shape[0] * rows.shape[1], weight.shape[1]), jnp.bfloat16),
        compiler_params=room(4),
        name=name,
    )(held(rows), held(weight))


def swap_over_kv(payload):
    return lax.all_to_all(payload, "kv", 0, 0, tiled=True)


def over_tp(mine):
    count = lax.axis_size("tp")
    parts = [mine]
    for step in range(1, count):
        swaps = [(place, place ^ step) for place in range(count)]
        parts.append(lax.ppermute(mine, "tp", swaps))
    return parts


def body(
    tokens,
    norm_gain,
    query_weight,
    key_weight,
    value_weight,
    gate_weight,
    beta_weight,
    decay_weight,
    decay_rate,
    head_gain,
    carried_state,
    block_keys,
    block_values,
    block_beta,
    block_decay,
    live_count,
    out_weight,
    mlp_gain,
    up_weight,
    down_weight,
):
    kv_index = lax.axis_index("kv")
    tp_index = lax.axis_index("tp")
    parts = lax.axis_size("kv")
    seqs, heads = carried_state.shape[:2]
    payload = project(
        kv_index,
        parts,
        tokens,
        norm_gain,
        [query_weight, key_weight, value_weight, gate_weight],
        beta_weight,
        decay_weight,
    )
    arrived = swap_over_kv(payload)
    state = block_state(
        live_count, block_keys, block_values, block_beta, block_decay, carried_state
    )
    copies, update, columns, fade = newest(
        tp_index, decay_rate, arrived, state, head_gain, heads, beta_weight.shape[1]
    )
    new_state = refresh(state, update, columns, fade, seqs)
    attended = over_tp(narrow(swap_over_kv(copies), out_weight, "attend"))
    residual = tokens.astype(jnp.float32) + sum(part.astype(jnp.float32) for part in attended)
    residual = residual.astype(jnp.bfloat16)
    gain = lax.dynamic_slice_in_dim(mlp_gain, kv_index * tokens.shape[1], tokens.shape[1], 0)
    scaled = (residual.astype(jnp.float32) * gain).astype(jnp.bfloat16)
    hidden = activate(swap_over_kv(widen(parts, residual, scaled, up_weight)))
    shares = over_tp(narrow(swap_over_kv(hidden), down_weight, "narrow"))
    mixed = residual.astype(jnp.float32) + sum(share.astype(jnp.float32) for share in shares)
    return (mixed.astype(jnp.bfloat16), new_state)


def solution(mesh):
    placed = (
        P(None, "kv"),
        P("kv"),
        P("kv", "tp"),
        P("kv", "tp"),
        P("kv", "tp"),
        P("kv", "tp"),
        P(),
        P(),
        P("tp"),
        P(),
        P("kv", "tp", None, None),
        P("kv", "tp", None, None),
        P("kv", "tp", None, None),
        P("kv", "tp", None),
        P("kv", "tp", None),
        P("kv"),
        P("tp", "kv"),
        P(),
        P("kv", "tp"),
        P("tp", "kv"),
    )
    return jax.shard_map(
        body,
        mesh=mesh,
        in_specs=placed,
        out_specs=(P(None, "kv"), P("kv", "tp", None, None)),
        check_vma=False,
    )
```

```python
import functools

import jax
import jax.numpy as jnp
from jax import lax
from jax.experimental import pallas as pl
from jax.experimental.pallas import tpu as pltpu
from jax.sharding import PartitionSpec as P

MODEL = 2048
EPS = 1e-06
LANES = 128
VMEM = pltpu.VMEM
SMEM = pltpu.SMEM


def in_vmem():
    return pl.BlockSpec(memory_space=VMEM)


def room(megabytes):
    return pltpu.CompilerParams(vmem_limit_bytes=megabytes << 20)


def held(value):
    return pltpu.with_memory_space_constraint(value, VMEM)


def afar(value):
    return pltpu.with_memory_space_constraint(value, pltpu.HBM)


def in_smem():
    return pl.BlockSpec(memory_space=SMEM)


def dot(left, right, contract=((1,), (0,)), precision=None):
    return lax.dot_general(
        left,
        right,
        (contract, ((), ())),
        precision=precision,
        preferred_element_type=jnp.float32,
    )


def halves(value):
    high = value.astype(jnp.bfloat16).astype(jnp.float32)
    return high, value - high


def project_kernel(
    tokens_ref,
    gain_ref,
    beta_ref,
    decay_ref,
    mlp_gain_ref,
    *rest,
    count,
    extras,
    sliced,
):
    far, rest = rest[:count], rest[count:]
    far_extras, rest = rest[:extras], rest[extras:]
    (out_ref, near_tokens_ref, near_mlp_gain_ref), rest = rest[:3], rest[3:]
    near_extras, rest = rest[:extras], rest[extras:]
    (gain_row, beta_rows, decay_rows), rest = rest[:3], rest[3:]
    near, semaphore = rest[:count], rest[count]
    columns = tokens_ref.shape[1]
    part = pl.ds(0 if sliced else lax.axis_index("kv") * columns, columns)
    pairs = [
        (tokens_ref, near_tokens_ref),
        (gain_ref, gain_row),
        (beta_ref.at[:, part], beta_rows),
        (decay_ref.at[:, part], decay_rows),
    ]
    pairs += list(zip(far, near)) + list(zip(far_extras, near_extras))
    pairs.append((mlp_gain_ref.at[:, part], near_mlp_gain_ref))
    copies = [
        pltpu.make_async_copy(source, target, semaphore.at[i])
        for i, (source, target) in enumerate(pairs)
    ]
    for copy in copies:
        copy.start()
    for copy in copies[:4]:
        copy.wait()
    parts, rows, _ = out_ref.shape
    tokens = near_tokens_ref[...].astype(jnp.float32)
    batch = tokens.shape[0]
    normed = (tokens * gain_row[...]).astype(jnp.bfloat16)
    squares = jnp.sum(tokens * tokens, axis=1, keepdims=True)
    heads = beta_rows.shape[0]
    small = jnp.concatenate(
        [
            beta_rows[...],
            decay_rows[...],
            jnp.zeros((LANES - 2 * heads, columns), jnp.bfloat16),
        ],
        axis=0,
    )
    gating = dot(normed, small, ((1,), (1,)))
    lane = lax.broadcasted_iota(jnp.int32, (batch, LANES), 1)
    high, low = halves(gating)
    square_high, square_low = halves(squares)
    tile = high + pltpu.roll(low, 2 * heads, axis=1)
    tile = jnp.where(lane == 4 * heads, square_high, tile)
    tile = jnp.where(lane == 4 * heads + 1, square_low, tile)
    width = near[0].shape[1]
    out_ref[:, :, count * width :] = tile.reshape(parts, rows, LANES).astype(jnp.bfloat16)
    for i in range(count):
        copies[4 + i].wait()
        made = dot(normed, near[i][...])
        out_ref[:, :, i * width : (i + 1) * width] = made.reshape(parts, rows, width).astype(
            jnp.bfloat16
        )
    for copy in copies[4 + count :]:
        copy.wait()


def project(parts, tokens, norm_gain, weights, beta_weight, decay_weight, mlp_gain, extras):
    batch, columns = tokens.shape
    width = weights[0].shape[1]
    count = len(weights)
    by_feature = [beta_weight.T, decay_weight.T, mlp_gain.reshape(1, -1)]
    heads = beta_weight.shape[1]
    sliced = bool(columns % LANES)
    if sliced:
        start = lax.axis_index("kv") * columns
        by_feature = [lax.dynamic_slice_in_dim(w, start, columns, 1) for w in by_feature]
    return pl.pallas_call(
        functools.partial(project_kernel, count=count, extras=len(extras), sliced=sliced),
        in_specs=[pl.BlockSpec(memory_space=pl.ANY)] * (5 + count + len(extras)),
        out_specs=[in_vmem()] * (3 + len(extras)),
        out_shape=[
            VMEM((parts, batch // parts, count * width + LANES), jnp.bfloat16),
            VMEM((batch, columns), jnp.bfloat16),
            VMEM((1, columns), jnp.float32),
        ]
        + [VMEM(extra.shape, extra.dtype) for extra in extras],
        scratch_shapes=[
            VMEM((1, columns), jnp.float32),
            VMEM((heads, columns), jnp.bfloat16),
            VMEM((heads, columns), jnp.bfloat16),
        ]
        + [VMEM((columns, width), jnp.bfloat16)] * count
        + [pltpu.SemaphoreType.DMA((5 + count + len(extras),))],
        compiler_params=room(4),
        name="project",
    )(
        afar(tokens),
        afar(norm_gain.reshape(1, columns)),
        *[afar(value) for value in by_feature + list(weights) + list(extras)],
    )


def block_kernel(
    live_ref,
    keys_ref,
    values_ref,
    betas_ref,
    decays_ref,
    far_state_ref,
    out_ref,
    state_ref,
    semaphore,
    *,
    heads,
    pack,
):
    pairs, slots, width = keys_ref.shape
    fetch = pltpu.make_async_copy(far_state_ref, state_ref, semaphore)
    fetch.start()
    owner_row = lax.broadcasted_iota(jnp.int32, (pairs, slots), 0) // heads
    limit = jnp.zeros((pairs, slots), jnp.int32)
    for s in range(pairs // heads):
        limit = jnp.where(owner_row == s, live_ref[:, s : s + 1] - 1, limit)
    pending = lax.broadcasted_iota(jnp.int32, (pairs, slots), 1) < limit
    betas = jnp.where(pending, betas_ref[...], 0.0)
    decays = jnp.where(pending, decays_ref[...], 0.0)
    upto = (
        lax.broadcasted_iota(jnp.int32, (slots, slots), 0)
        <= lax.broadcasted_iota(jnp.int32, (slots, slots), 1)
    ).astype(jnp.float32)
    totals = dot(decays, upto, precision=lax.Precision.HIGHEST)
    columns = jnp.concatenate([totals, betas], axis=0).T
    total_columns = columns[:, :pairs]
    beta_columns = columns[:, pairs:]
    ending = total_columns[slots - 1 : slots, :]
    grown = jnp.exp(total_columns)
    faded = jnp.exp(ending - total_columns)
    whole_fade = jnp.exp(totals[:, slots - 1 : slots])
    across = pack * slots
    row = lax.broadcasted_iota(jnp.int32, (slots, across), 0)
    lane = lax.broadcasted_iota(jnp.int32, (slots, across), 1)
    column = lane % slots
    owner = lane // slots
    strict = row > column
    identity = (row == column).astype(jnp.float32)
    sizes = []
    size = 1
    while size < slots:
        sizes.append(size)
        size *= 2
    joins = [(row // (2 * s) == column // (2 * s)) & (row // s != column // s) for s in sizes]

    def choose(pieces):
        chosen = pieces[-1]
        for m in range(pack - 2, -1, -1):
            chosen = jnp.where(owner == m, pieces[m], chosen)
        return chosen

    def spread_out(value):
        return jnp.concatenate(
            [jnp.where(owner == m, value, 0.0).astype(jnp.bfloat16) for m in range(pack)], axis=0
        )

    packs = range(pairs // pack)
    lower = []
    inverse = []
    for g in packs:
        members = range(g * pack, (g + 1) * pack)
        stacked = keys_ref[g * pack : (g + 1) * pack].reshape(across, width)
        overlaps = dot(stacked, stacked, ((1,), (1,)))
        overlap = choose([overlaps[m * slots : (m + 1) * slots] for m in range(pack)])
        along = jnp.concatenate([totals[p : p + 1, :] for p in members], axis=1)
        down = choose([total_columns[:, p : p + 1] for p in members])
        beta = choose([beta_columns[:, p : p + 1] for p in members])
        weight = jnp.exp(jnp.where(strict, down - along, 0.0))
        lower.append(jnp.where(strict, beta * overlap * weight, 0.0))
        inverse.append(identity - jnp.where(joins[0], lower[g], 0.0))
    for level in range(1, len(sizes)):
        middle = [
            dot(
                inverse[g].astype(jnp.bfloat16),
                spread_out(jnp.where(joins[level], lower[g], 0.0)),
            )
            for g in packs
        ]
        for g in packs:
            inverse[g] = inverse[g] - dot(middle[g].astype(jnp.bfloat16), spread_out(inverse[g]))
    fetch.wait()
    for g in packs:
        members = range(g * pack, (g + 1) * pack)
        wanted = []
        for p in members:
            recalled = dot(keys_ref[p], state_ref[p].astype(jnp.bfloat16))
            wanted.append(
                beta_columns[:, p : p + 1]
                * (values_ref[p].astype(jnp.float32) - grown[:, p : p + 1] * recalled)
            )
        wanted = jnp.concatenate(wanted, axis=0).astype(jnp.bfloat16)
        updates = dot(spread_out(inverse[g]), wanted)
        for m, p in enumerate(members):
            update = faded[:, p : p + 1] * updates[m * slots : (m + 1) * slots]
            made = dot(keys_ref[p], update.astype(jnp.bfloat16), ((0,), (0,)))
            out_ref[p] = whole_fade[p : p + 1, :] * state_ref[p] + made


def block_state(live_count, keys, values, betas, decays, state, pack=4):
    seqs, heads, slots, width = keys.shape
    pairs = seqs * heads
    return pl.pallas_call(
        functools.partial(block_kernel, heads=heads, pack=pack),
        in_specs=[in_vmem()] * 5 + [pl.BlockSpec(memory_space=pl.ANY)],
        out_specs=in_vmem(),
        scratch_shapes=[VMEM((pairs, width, width), jnp.float32), pltpu.SemaphoreType.DMA],
        out_shape=VMEM((pairs, width, width), jnp.float32),
        cost_estimate=pl.CostEstimate(
            flops=60_000_000, bytes_accessed=5_000_000, transcendentals=0
        ),
        compiler_params=room(24),
        name="block_state",
    )(
        held(live_count),
        held(keys.reshape(pairs, slots, width)),
        held(values.reshape(pairs, slots, width)),
        held(betas),
        held(decays),
        afar(state.reshape(pairs, width, width)),
    )


def newest_kernel(
    rate_ref,
    arrived_ref,
    state_ref,
    gain_ref,
    mixed_ref,
    update_ref,
    columns_ref,
    fade_ref,
    recalled_ref,
    answered_ref,
    *,
    heads,
    total_heads,
):
    seqs = arrived_ref.shape[1]
    width = state_ref.shape[1]
    summed = jnp.sum(arrived_ref[...].astype(jnp.float32), axis=0)
    raw = lambda i, h: summed[:, (i * heads + h) * width : (i * heads + h + 1) * width]
    key_and_query = [raw(1, h) for h in range(heads)] + [raw(0, h) for h in range(heads)]
    columns = jnp.concatenate(key_and_query, axis=0).T
    columns_ref[...] = columns
    lines = [
        jnp.concatenate([raw(1, h), raw(0, h)], axis=0).astype(jnp.bfloat16) for h in range(heads)
    ]
    for h in range(heads):
        for s in range(seqs):
            found = dot(lines[h], state_ref[s * heads + h].astype(jnp.bfloat16))
            j = h * seqs + s
            recalled_ref[j : j + 1, :] = found[s : s + 1, :]
            answered_ref[j : j + 1, :] = found[seqs + s : seqs + s + 1, :]
    tail = summed[:, 4 * heads * width :]
    lane = lax.broadcasted_iota(jnp.int32, (seqs, LANES), 1)
    is_square = (lane == 4 * total_heads) | (lane == 4 * total_heads + 1)
    squares = jnp.sum(jnp.where(is_square, tail, 0.0), axis=1, keepdims=True)
    scale = lax.rsqrt(squares / MODEL + EPS)
    gating = (tail + pltpu.roll(tail, LANES - 2 * total_heads, axis=1)) * scale
    first = lax.axis_index("tp") * heads
    pick = lambda at: jnp.sum(jnp.where(lane == at, gating, 0.0), axis=1, keepdims=True)
    for h in range(heads):
        beta = jax.nn.sigmoid(pick(first + h))
        before = pick(total_heads + first + h)
        softplus = jnp.maximum(before, 0.0) + jnp.log1p(jnp.exp(-jnp.abs(before)))
        fade = jnp.exp(-rate_ref[:, h : h + 1] * softplus)
        rows = slice(h * seqs, (h + 1) * seqs)
        key = raw(1, h) * scale
        key_scale = lax.rsqrt(jnp.sum(key * key, axis=1, keepdims=True) + EPS)
        query = raw(0, h) * scale
        agreement = jnp.sum(key * query, axis=1, keepdims=True) * key_scale
        value = raw(2, h) * scale
        gate = raw(3, h) * scale
        update = beta * (value - fade * (key_scale * scale) * recalled_ref[rows, :])
        readout = fade * scale * answered_ref[rows, :] + agreement * update
        power = jnp.mean(readout * readout, axis=1, keepdims=True)
        mixed = readout * lax.rsqrt(power + EPS) * gain_ref[...] * (gate * jax.nn.sigmoid(gate))
        shape = (mixed_ref.shape[0], seqs, width)
        mixed_ref[:, :, h * width : (h + 1) * width] = jnp.broadcast_to(mixed[None], shape).astype(
            jnp.bfloat16
        )
        update_ref[rows, :] = update * (key_scale * scale)
        fade_ref[rows, :] = jnp.broadcast_to(fade, (seqs, width))


def newest(decay_rate, arrived, state, head_gain, heads, total_heads):
    parts, seqs, _ = arrived.shape
    width = state.shape[1]
    count = heads * seqs
    return pl.pallas_call(
        functools.partial(newest_kernel, heads=heads, total_heads=total_heads),
        in_specs=[in_vmem()] * 4,
        out_specs=[in_vmem()] * 4,
        out_shape=[
            VMEM((parts, seqs, heads * width), jnp.bfloat16),
            VMEM((count, width), jnp.float32),
            VMEM((width, 2 * count), jnp.float32),
            VMEM((count, width), jnp.float32),
        ],
        scratch_shapes=[pltpu.VMEM((count, width), jnp.float32)] * 2,
        compiler_params=room(4),
        name="newest",
    )(
        held(decay_rate),
        held(arrived),
        held(state),
        held(head_gain),
    )


def refresh_kernel(state_ref, update_ref, columns_ref, fade_ref, out_ref, made_ref, semaphore):
    pairs = state_ref.shape[0]
    seqs = made_ref.shape[0]
    heads = pairs // seqs
    columns = columns_ref[...]
    copies = []
    for s in range(seqs):
        for h in range(heads):
            j = h * seqs + s
            made_ref[s, h] = (
                fade_ref[j : j + 1, :] * state_ref[s * heads + h]
                + columns[:, j : j + 1] * update_ref[j : j + 1, :]
            )
        copies.append(pltpu.make_async_copy(made_ref.at[s], out_ref.at[s], semaphore.at[s]))
        copies[-1].start()
    for copy in copies:
        copy.wait()


def refresh(state, update, columns, fade, seqs):
    pairs, width, _ = state.shape
    shape = (seqs, pairs // seqs, width, width)
    return pl.pallas_call(
        refresh_kernel,
        in_specs=[in_vmem()] * 4,
        out_specs=pl.BlockSpec(memory_space=pl.ANY),
        out_shape=jax.ShapeDtypeStruct(shape, jnp.float32),
        scratch_shapes=[pltpu.VMEM(shape, jnp.float32), pltpu.SemaphoreType.DMA((seqs,))],
        cost_estimate=pl.CostEstimate(
            flops=10_000_000, bytes_accessed=4_000_000, transcendentals=0
        ),
        compiler_params=room(8),
        name="refresh",
    )(held(state), held(update), held(columns), held(fade))


def widen_kernel(residual_ref, scaled_ref, weight_ref, out_ref):
    parts, rows, _ = out_ref.shape
    value = residual_ref[...].astype(jnp.float32)
    batch = value.shape[0]
    high, low = halves(jnp.sum(value * value, axis=1, keepdims=True))
    lane = lax.broadcasted_iota(jnp.int32, (batch, LANES), 1)
    tile = jnp.where(lane == 0, high, jnp.where(lane == 1, low, 0.0))
    units = weight_ref.shape[1]
    out_ref[:, :, units:] = tile.reshape(parts, rows, LANES).astype(jnp.bfloat16)
    made = dot(scaled_ref[...], weight_ref[...])
    out_ref[:, :, :units] = made.reshape(parts, rows, units).astype(jnp.bfloat16)


def widen(parts, residual, scaled, up_weight):
    batch = residual.shape[0]
    units = up_weight.shape[1]
    return pl.pallas_call(
        widen_kernel,
        in_specs=[in_vmem()] * 3,
        out_specs=in_vmem(),
        out_shape=VMEM((parts, batch // parts, units + LANES), jnp.bfloat16),
        compiler_params=room(6),
        name="widen",
    )(held(residual), held(scaled), held(up_weight))


def activate_kernel(arrived_ref, out_ref):
    units = out_ref.shape[2]
    summed = jnp.sum(arrived_ref[...].astype(jnp.float32), axis=0)
    tail = summed[:, units:]
    lane = lax.broadcasted_iota(jnp.int32, tail.shape, 1)
    squares = jnp.sum(jnp.where(lane < 2, tail, 0.0), axis=1, keepdims=True)
    scale = lax.rsqrt(squares / MODEL + EPS)
    hidden = jnp.square(jnp.maximum(summed[:, :units] * scale, 0.0))
    out_ref[...] = jnp.broadcast_to(hidden[None], out_ref.shape).astype(jnp.bfloat16)


def activate(arrived):
    parts, seqs, wide = arrived.shape
    return pl.pallas_call(
        activate_kernel,
        in_specs=[in_vmem()],
        out_specs=in_vmem(),
        out_shape=VMEM((parts, seqs, wide - LANES), jnp.bfloat16),
        compiler_params=room(4),
        name="activate",
    )(held(arrived))


def narrow_kernel(rows_ref, weight_ref, out_ref):
    rows = rows_ref[...]
    rows = rows.reshape(rows.shape[0] * rows.shape[1], rows.shape[2])
    out_ref[...] = dot(rows, weight_ref[...]).astype(jnp.bfloat16)


def narrow(rows, weight, name):
    return pl.pallas_call(
        narrow_kernel,
        in_specs=[in_vmem()] * 2,
        out_specs=in_vmem(),
        out_shape=VMEM((rows.shape[0] * rows.shape[1], weight.shape[1]), jnp.bfloat16),
        compiler_params=room(4),
        name=name,
    )(held(rows), held(weight))


def swap_over_kv(payload):
    return lax.all_to_all(payload, "kv", 0, 0, tiled=True)


def over_tp(mine):
    count = lax.axis_size("tp")
    parts = [mine]
    for step in range(1, count):
        swaps = [(place, place ^ step) for place in range(count)]
        parts.append(lax.ppermute(mine, "tp", swaps))
    return parts


def body(
    tokens,
    norm_gain,
    query_weight,
    key_weight,
    value_weight,
    gate_weight,
    beta_weight,
    decay_weight,
    decay_rate,
    head_gain,
    carried_state,
    block_keys,
    block_values,
    block_beta,
    block_decay,
    live_count,
    out_weight,
    mlp_gain,
    up_weight,
    down_weight,
):
    parts = lax.axis_size("kv")
    seqs, heads, slots, width = block_keys.shape
    pairs = seqs * heads
    payload, near_tokens, gain, live, betas, decays, rates, head_gains = project(
        parts,
        tokens,
        norm_gain,
        [query_weight, key_weight, value_weight, gate_weight],
        beta_weight,
        decay_weight,
        mlp_gain,
        [
            live_count.reshape(1, seqs),
            block_beta.reshape(pairs, slots),
            block_decay.reshape(pairs, slots),
            decay_rate.reshape(1, heads),
            head_gain.reshape(1, width),
        ],
    )
    arrived = swap_over_kv(payload)
    state = block_state(live, block_keys, block_values, betas, decays, carried_state)
    copies, update, columns, fade = newest(
        rates, arrived, state, head_gains, heads, beta_weight.shape[1]
    )
    new_state = refresh(state, update, columns, fade, seqs)
    attended = over_tp(narrow(swap_over_kv(copies), out_weight, "attend"))
    residual = near_tokens.astype(jnp.float32) + sum(part.astype(jnp.float32) for part in attended)
    residual = residual.astype(jnp.bfloat16)
    scaled = (residual.astype(jnp.float32) * gain).astype(jnp.bfloat16)
    hidden = activate(swap_over_kv(widen(parts, residual, scaled, up_weight)))
    shares = over_tp(narrow(swap_over_kv(hidden), down_weight, "narrow"))
    mixed = residual.astype(jnp.float32) + sum(share.astype(jnp.float32) for share in shares)
    return (mixed.astype(jnp.bfloat16), new_state)


def solution(mesh):
    placed = (
        P(None, "kv"),
        P("kv"),
        P("kv", "tp"),
        P("kv", "tp"),
        P("kv", "tp"),
        P("kv", "tp"),
        P(),
        P(),
        P("tp"),
        P(),
        P("kv", "tp", None, None),
        P("kv", "tp", None, None),
        P("kv", "tp", None, None),
        P("kv", "tp", None),
        P("kv", "tp", None),
        P("kv"),
        P("tp", "kv"),
        P(),
        P("kv", "tp"),
        P("tp", "kv"),
    )
    return jax.shard_map(
        body,
        mesh=mesh,
        in_specs=placed,
        out_specs=(P(None, "kv"), P("kv", "tp", None, None)),
        check_vma=False,
    )
```

```python
import functools

import jax
import jax.numpy as jnp
from jax import lax
from jax.experimental import pallas as pl
from jax.experimental.pallas import tpu as pltpu
from jax.sharding import PartitionSpec as P

MODEL = 2048
EPS = 1e-06
LANES = 128
VMEM = pltpu.VMEM
SMEM = pltpu.SMEM


def in_vmem():
    return pl.BlockSpec(memory_space=VMEM)


def room(megabytes):
    return pltpu.CompilerParams(vmem_limit_bytes=megabytes << 20)


def held(value):
    return pltpu.with_memory_space_constraint(value, VMEM)


def afar(value):
    return pltpu.with_memory_space_constraint(value, pltpu.HBM)


def in_smem():
    return pl.BlockSpec(memory_space=SMEM)


def dot(left, right, contract=((1,), (0,)), precision=None):
    return lax.dot_general(
        left,
        right,
        (contract, ((), ())),
        precision=precision,
        preferred_element_type=jnp.float32,
    )


def halves(value):
    high = value.astype(jnp.bfloat16).astype(jnp.float32)
    return high, value - high


def exchange_order(parts):
    stride = 3 if parts % 3 else 1
    return [(parts // 2 + 1 + stride * i) % parts for i in range(parts)]


def deal(out_ref, lanes, value):
    parts, rows, _ = out_ref.shape
    for slot, place in enumerate(exchange_order(parts)):
        out_ref[slot, :, lanes] = value[place * rows : (place + 1) * rows].astype(jnp.bfloat16)


def project_kernel(
    tokens_ref,
    gain_ref,
    beta_ref,
    decay_ref,
    mlp_gain_ref,
    *rest,
    count,
    extras,
    sliced,
):
    far, rest = rest[:count], rest[count:]
    far_extras, rest = rest[:extras], rest[extras:]
    (out_ref, near_tokens_ref, near_mlp_gain_ref), rest = rest[:3], rest[3:]
    near_extras, rest = rest[:extras], rest[extras:]
    (gain_row, beta_rows, decay_rows), rest = rest[:3], rest[3:]
    near, semaphore = rest[:count], rest[count]
    columns = tokens_ref.shape[1]
    part = pl.ds(0 if sliced else lax.axis_index("kv") * columns, columns)
    pairs = [
        (tokens_ref, near_tokens_ref),
        (gain_ref, gain_row),
        (beta_ref.at[:, part], beta_rows),
        (decay_ref.at[:, part], decay_rows),
    ]
    pairs += list(zip(far, near)) + list(zip(far_extras, near_extras))
    pairs.append((mlp_gain_ref.at[:, part], near_mlp_gain_ref))
    copies = [
        pltpu.make_async_copy(source, target, semaphore.at[i])
        for i, (source, target) in enumerate(pairs)
    ]
    for copy in copies:
        copy.start()
    for copy in copies[:4]:
        copy.wait()
    tokens = near_tokens_ref[...].astype(jnp.float32)
    batch = tokens.shape[0]
    normed = (tokens * gain_row[...]).astype(jnp.bfloat16)
    squares = jnp.sum(tokens * tokens, axis=1, keepdims=True)
    heads = beta_rows.shape[0]
    small = jnp.concatenate(
        [
            beta_rows[...],
            decay_rows[...],
            jnp.zeros((LANES - 2 * heads, columns), jnp.bfloat16),
        ],
        axis=0,
    )
    gating = dot(normed, small, ((1,), (1,)))
    lane = lax.broadcasted_iota(jnp.int32, (batch, LANES), 1)
    high, low = halves(gating)
    square_high, square_low = halves(squares)
    tile = high + pltpu.roll(low, 2 * heads, axis=1)
    tile = jnp.where(lane == 4 * heads, square_high, tile)
    tile = jnp.where(lane == 4 * heads + 1, square_low, tile)
    width = near[0].shape[1]
    deal(out_ref, slice(count * width, count * width + LANES), tile)
    for i in range(count):
        copies[4 + i].wait()
        deal(out_ref, slice(i * width, (i + 1) * width), dot(normed, near[i][...]))
    for copy in copies[4 + count :]:
        copy.wait()


def project(parts, tokens, norm_gain, weights, beta_weight, decay_weight, mlp_gain, extras):
    batch, columns = tokens.shape
    width = weights[0].shape[1]
    count = len(weights)
    by_feature = [beta_weight.T, decay_weight.T, mlp_gain.reshape(1, -1)]
    heads = beta_weight.shape[1]
    sliced = bool(columns % LANES)
    if sliced:
        start = lax.axis_index("kv") * columns
        by_feature = [lax.dynamic_slice_in_dim(w, start, columns, 1) for w in by_feature]
    return pl.pallas_call(
        functools.partial(project_kernel, count=count, extras=len(extras), sliced=sliced),
        in_specs=[pl.BlockSpec(memory_space=pl.ANY)] * (5 + count + len(extras)),
        out_specs=[in_vmem()] * (3 + len(extras)),
        out_shape=[
            VMEM((parts, batch // parts, count * width + LANES), jnp.bfloat16),
            VMEM((batch, columns), jnp.bfloat16),
            VMEM((1, columns), jnp.float32),
        ]
        + [VMEM(extra.shape, extra.dtype) for extra in extras],
        scratch_shapes=[
            VMEM((1, columns), jnp.float32),
            VMEM((heads, columns), jnp.bfloat16),
            VMEM((heads, columns), jnp.bfloat16),
        ]
        + [VMEM((columns, width), jnp.bfloat16)] * count
        + [pltpu.SemaphoreType.DMA((5 + count + len(extras),))],
        compiler_params=room(4),
        name="project",
    )(
        afar(tokens),
        afar(norm_gain.reshape(1, columns)),
        *[afar(value) for value in by_feature + list(weights) + list(extras)],
    )


def block_kernel(
    live_ref,
    keys_ref,
    values_ref,
    betas_ref,
    decays_ref,
    far_state_ref,
    out_ref,
    state_ref,
    semaphore,
    *,
    heads,
    pack,
):
    pairs, slots, width = keys_ref.shape
    fetch = pltpu.make_async_copy(far_state_ref, state_ref, semaphore)
    fetch.start()
    owner_row = lax.broadcasted_iota(jnp.int32, (pairs, slots), 0) // heads
    limit = jnp.zeros((pairs, slots), jnp.int32)
    for s in range(pairs // heads):
        limit = jnp.where(owner_row == s, live_ref[:, s : s + 1] - 1, limit)
    pending = lax.broadcasted_iota(jnp.int32, (pairs, slots), 1) < limit
    betas = jnp.where(pending, betas_ref[...], 0.0)
    decays = jnp.where(pending, decays_ref[...], 0.0)
    upto = (
        lax.broadcasted_iota(jnp.int32, (slots, slots), 0)
        <= lax.broadcasted_iota(jnp.int32, (slots, slots), 1)
    ).astype(jnp.float32)
    totals = dot(decays, upto, precision=lax.Precision.HIGHEST)
    columns = jnp.concatenate([totals, betas], axis=0).T
    total_columns = columns[:, :pairs]
    beta_columns = columns[:, pairs:]
    ending = total_columns[slots - 1 : slots, :]
    grown = jnp.exp(total_columns)
    faded = jnp.exp(ending - total_columns)
    whole_fade = jnp.exp(totals[:, slots - 1 : slots])
    across = pack * slots
    row = lax.broadcasted_iota(jnp.int32, (slots, across), 0)
    lane = lax.broadcasted_iota(jnp.int32, (slots, across), 1)
    column = lane % slots
    owner = lane // slots
    strict = row > column
    identity = (row == column).astype(jnp.float32)
    sizes = []
    size = 1
    while size < slots:
        sizes.append(size)
        size *= 2
    joins = [(row // (2 * s) == column // (2 * s)) & (row // s != column // s) for s in sizes]

    def choose(pieces):
        chosen = pieces[-1]
        for m in range(pack - 2, -1, -1):
            chosen = jnp.where(owner == m, pieces[m], chosen)
        return chosen

    def spread_out(value):
        return jnp.concatenate(
            [jnp.where(owner == m, value, 0.0).astype(jnp.bfloat16) for m in range(pack)], axis=0
        )

    packs = range(pairs // pack)
    lower = []
    inverse = []
    for g in packs:
        members = range(g * pack, (g + 1) * pack)
        stacked = keys_ref[g * pack : (g + 1) * pack].reshape(across, width)
        overlaps = dot(stacked, stacked, ((1,), (1,)))
        overlap = choose([overlaps[m * slots : (m + 1) * slots] for m in range(pack)])
        along = jnp.concatenate([totals[p : p + 1, :] for p in members], axis=1)
        down = choose([total_columns[:, p : p + 1] for p in members])
        beta = choose([beta_columns[:, p : p + 1] for p in members])
        weight = jnp.exp(jnp.where(strict, down - along, 0.0))
        lower.append(jnp.where(strict, beta * overlap * weight, 0.0))
        inverse.append(identity - jnp.where(joins[0], lower[g], 0.0))
    for level in range(1, len(sizes)):
        middle = [
            dot(
                inverse[g].astype(jnp.bfloat16),
                spread_out(jnp.where(joins[level], lower[g], 0.0)),
            )
            for g in packs
        ]
        for g in packs:
            inverse[g] = inverse[g] - dot(middle[g].astype(jnp.bfloat16), spread_out(inverse[g]))
    fetch.wait()
    for g in packs:
        members = range(g * pack, (g + 1) * pack)
        wanted = []
        for p in members:
            recalled = dot(keys_ref[p], state_ref[p].astype(jnp.bfloat16))
            wanted.append(
                beta_columns[:, p : p + 1]
                * (values_ref[p].astype(jnp.float32) - grown[:, p : p + 1] * recalled)
            )
        wanted = jnp.concatenate(wanted, axis=0).astype(jnp.bfloat16)
        updates = dot(spread_out(inverse[g]), wanted)
        for m, p in enumerate(members):
            update = faded[:, p : p + 1] * updates[m * slots : (m + 1) * slots]
            made = dot(keys_ref[p], update.astype(jnp.bfloat16), ((0,), (0,)))
            out_ref[p] = whole_fade[p : p + 1, :] * state_ref[p] + made


def block_state(live_count, keys, values, betas, decays, state, pack=4):
    seqs, heads, slots, width = keys.shape
    pairs = seqs * heads
    return pl.pallas_call(
        functools.partial(block_kernel, heads=heads, pack=pack),
        in_specs=[in_vmem()] * 5 + [pl.BlockSpec(memory_space=pl.ANY)],
        out_specs=in_vmem(),
        scratch_shapes=[VMEM((pairs, width, width), jnp.float32), pltpu.SemaphoreType.DMA],
        out_shape=VMEM((pairs, width, width), jnp.float32),
        cost_estimate=pl.CostEstimate(
            flops=60_000_000, bytes_accessed=5_000_000, transcendentals=0
        ),
        compiler_params=room(24),
        name="block_state",
    )(
        held(live_count),
        held(keys.reshape(pairs, slots, width)),
        held(values.reshape(pairs, slots, width)),
        held(betas),
        held(decays),
        afar(state.reshape(pairs, width, width)),
    )


def newest_kernel(
    rate_ref,
    arrived_ref,
    state_ref,
    gain_ref,
    mixed_ref,
    update_ref,
    columns_ref,
    fade_ref,
    recalled_ref,
    answered_ref,
    *,
    heads,
    total_heads,
):
    seqs = arrived_ref.shape[1]
    width = state_ref.shape[1]
    summed = jnp.sum(arrived_ref[...].astype(jnp.float32), axis=0)
    raw = lambda i, h: summed[:, (i * heads + h) * width : (i * heads + h + 1) * width]
    key_and_query = [raw(1, h) for h in range(heads)] + [raw(0, h) for h in range(heads)]
    columns = jnp.concatenate(key_and_query, axis=0).T
    columns_ref[...] = columns
    lines = [
        jnp.concatenate([raw(1, h), raw(0, h)], axis=0).astype(jnp.bfloat16) for h in range(heads)
    ]
    for h in range(heads):
        for s in range(seqs):
            found = dot(lines[h], state_ref[s * heads + h].astype(jnp.bfloat16))
            j = h * seqs + s
            recalled_ref[j : j + 1, :] = found[s : s + 1, :]
            answered_ref[j : j + 1, :] = found[seqs + s : seqs + s + 1, :]
    tail = summed[:, 4 * heads * width :]
    lane = lax.broadcasted_iota(jnp.int32, (seqs, LANES), 1)
    is_square = (lane == 4 * total_heads) | (lane == 4 * total_heads + 1)
    squares = jnp.sum(jnp.where(is_square, tail, 0.0), axis=1, keepdims=True)
    scale = lax.rsqrt(squares / MODEL + EPS)
    gating = (tail + pltpu.roll(tail, LANES - 2 * total_heads, axis=1)) * scale
    first = lax.axis_index("tp") * heads
    pick = lambda at: jnp.sum(jnp.where(lane == at, gating, 0.0), axis=1, keepdims=True)
    for h in range(heads):
        beta = jax.nn.sigmoid(pick(first + h))
        before = pick(total_heads + first + h)
        softplus = jnp.maximum(before, 0.0) + jnp.log1p(jnp.exp(-jnp.abs(before)))
        fade = jnp.exp(-rate_ref[:, h : h + 1] * softplus)
        rows = slice(h * seqs, (h + 1) * seqs)
        key = raw(1, h) * scale
        key_scale = lax.rsqrt(jnp.sum(key * key, axis=1, keepdims=True) + EPS)
        query = raw(0, h) * scale
        agreement = jnp.sum(key * query, axis=1, keepdims=True) * key_scale
        value = raw(2, h) * scale
        gate = raw(3, h) * scale
        update = beta * (value - fade * (key_scale * scale) * recalled_ref[rows, :])
        readout = fade * scale * answered_ref[rows, :] + agreement * update
        power = jnp.mean(readout * readout, axis=1, keepdims=True)
        mixed = readout * lax.rsqrt(power + EPS) * gain_ref[...] * (gate * jax.nn.sigmoid(gate))
        shape = (mixed_ref.shape[0], seqs, width)
        mixed_ref[:, :, h * width : (h + 1) * width] = jnp.broadcast_to(mixed[None], shape).astype(
            jnp.bfloat16
        )
        update_ref[rows, :] = update * (key_scale * scale)
        fade_ref[rows, :] = jnp.broadcast_to(fade, (seqs, width))


def newest(decay_rate, arrived, state, head_gain, heads, total_heads):
    parts, seqs, _ = arrived.shape
    width = state.shape[1]
    count = heads * seqs
    return pl.pallas_call(
        functools.partial(newest_kernel, heads=heads, total_heads=total_heads),
        in_specs=[in_vmem()] * 4,
        out_specs=[in_vmem()] * 4,
        out_shape=[
            VMEM((parts, seqs, heads * width), jnp.bfloat16),
            VMEM((count, width), jnp.float32),
            VMEM((width, 2 * count), jnp.float32),
            VMEM((count, width), jnp.float32),
        ],
        scratch_shapes=[pltpu.VMEM((count, width), jnp.float32)] * 2,
        compiler_params=room(4),
        name="newest",
    )(
        held(decay_rate),
        held(arrived),
        held(state),
        held(head_gain),
    )


def refresh_kernel(state_ref, update_ref, columns_ref, fade_ref, out_ref, made_ref, semaphore):
    pairs = state_ref.shape[0]
    seqs = made_ref.shape[0]
    heads = pairs // seqs
    columns = columns_ref[...]
    copies = []
    for s in range(seqs):
        for h in range(heads):
            j = h * seqs + s
            made_ref[s, h] = (
                fade_ref[j : j + 1, :] * state_ref[s * heads + h]
                + columns[:, j : j + 1] * update_ref[j : j + 1, :]
            )
        copies.append(pltpu.make_async_copy(made_ref.at[s], out_ref.at[s], semaphore.at[s]))
        copies[-1].start()
    for copy in copies:
        copy.wait()


def refresh(state, update, columns, fade, seqs):
    pairs, width, _ = state.shape
    shape = (seqs, pairs // seqs, width, width)
    return pl.pallas_call(
        refresh_kernel,
        in_specs=[in_vmem()] * 4,
        out_specs=pl.BlockSpec(memory_space=pl.ANY),
        out_shape=jax.ShapeDtypeStruct(shape, jnp.float32),
        scratch_shapes=[pltpu.VMEM(shape, jnp.float32), pltpu.SemaphoreType.DMA((seqs,))],
        cost_estimate=pl.CostEstimate(
            flops=10_000_000, bytes_accessed=4_000_000, transcendentals=0
        ),
        compiler_params=room(8),
        name="refresh",
    )(held(state), held(update), held(columns), held(fade))


def widen_kernel(residual_ref, scaled_ref, weight_ref, out_ref):
    value = residual_ref[...].astype(jnp.float32)
    batch = value.shape[0]
    high, low = halves(jnp.sum(value * value, axis=1, keepdims=True))
    lane = lax.broadcasted_iota(jnp.int32, (batch, LANES), 1)
    tile = jnp.where(lane == 0, high, jnp.where(lane == 1, low, 0.0))
    units = weight_ref.shape[1]
    deal(out_ref, slice(units, units + LANES), tile)
    deal(out_ref, slice(0, units), dot(scaled_ref[...], weight_ref[...]))


def widen(parts, residual, scaled, up_weight):
    batch = residual.shape[0]
    units = up_weight.shape[1]
    return pl.pallas_call(
        widen_kernel,
        in_specs=[in_vmem()] * 3,
        out_specs=in_vmem(),
        out_shape=VMEM((parts, batch // parts, units + LANES), jnp.bfloat16),
        compiler_params=room(6),
        name="widen",
    )(held(residual), held(scaled), held(up_weight))


def activate_kernel(arrived_ref, out_ref):
    units = out_ref.shape[2]
    summed = jnp.sum(arrived_ref[...].astype(jnp.float32), axis=0)
    tail = summed[:, units:]
    lane = lax.broadcasted_iota(jnp.int32, tail.shape, 1)
    squares = jnp.sum(jnp.where(lane < 2, tail, 0.0), axis=1, keepdims=True)
    scale = lax.rsqrt(squares / MODEL + EPS)
    hidden = jnp.square(jnp.maximum(summed[:, :units] * scale, 0.0))
    out_ref[...] = jnp.broadcast_to(hidden[None], out_ref.shape).astype(jnp.bfloat16)


def activate(arrived):
    parts, seqs, wide = arrived.shape
    return pl.pallas_call(
        activate_kernel,
        in_specs=[in_vmem()],
        out_specs=in_vmem(),
        out_shape=VMEM((parts, seqs, wide - LANES), jnp.bfloat16),
        compiler_params=room(4),
        name="activate",
    )(held(arrived))


def narrow_kernel(rows_ref, weight_ref, out_ref):
    parts, rows, width = rows_ref.shape
    made = dot(rows_ref[...].reshape(parts * rows, width), weight_ref[...])
    order = exchange_order(parts)
    slots = [order.index(place) for place in range(parts)]
    pieces = [made[slot * rows : (slot + 1) * rows] for slot in slots]
    out_ref[...] = jnp.concatenate(pieces, axis=0).astype(jnp.bfloat16)


def narrow(rows, weight, name):
    return pl.pallas_call(
        narrow_kernel,
        in_specs=[in_vmem()] * 2,
        out_specs=in_vmem(),
        out_shape=VMEM((rows.shape[0] * rows.shape[1], weight.shape[1]), jnp.bfloat16),
        compiler_params=room(4),
        name=name,
    )(held(rows), held(weight))


def swap_over_kv(payload):
    groups = [exchange_order(payload.shape[0])]
    return lax.all_to_all(payload, "kv", 0, 0, axis_index_groups=groups, tiled=True)


def over_tp(mine):
    count = lax.axis_size("tp")
    parts = [mine]
    for step in range(1, count):
        swaps = [(place, place ^ step) for place in range(count)]
        parts.append(lax.ppermute(mine, "tp", swaps))
    return parts


def body(
    tokens,
    norm_gain,
    query_weight,
    key_weight,
    value_weight,
    gate_weight,
    beta_weight,
    decay_weight,
    decay_rate,
    head_gain,
    carried_state,
    block_keys,
    block_values,
    block_beta,
    block_decay,
    live_count,
    out_weight,
    mlp_gain,
    up_weight,
    down_weight,
):
    parts = lax.axis_size("kv")
    seqs, heads, slots, width = block_keys.shape
    pairs = seqs * heads
    payload, near_tokens, gain, live, betas, decays, rates, head_gains = project(
        parts,
        tokens,
        norm_gain,
        [query_weight, key_weight, value_weight, gate_weight],
        beta_weight,
        decay_weight,
        mlp_gain,
        [
            live_count.reshape(1, seqs),
            block_beta.reshape(pairs, slots),
            block_decay.reshape(pairs, slots),
            decay_rate.reshape(1, heads),
            head_gain.reshape(1, width),
        ],
    )
    arrived = swap_over_kv(payload)
    state = block_state(live, block_keys, block_values, betas, decays, carried_state)
    copies, update, columns, fade = newest(
        rates, arrived, state, head_gains, heads, beta_weight.shape[1]
    )
    new_state = refresh(state, update, columns, fade, seqs)
    attended = over_tp(narrow(swap_over_kv(copies), out_weight, "attend"))
    residual = near_tokens.astype(jnp.float32) + sum(part.astype(jnp.float32) for part in attended)
    residual = residual.astype(jnp.bfloat16)
    scaled = (residual.astype(jnp.float32) * gain).astype(jnp.bfloat16)
    hidden = activate(swap_over_kv(widen(parts, residual, scaled, up_weight)))
    shares = over_tp(narrow(swap_over_kv(hidden), down_weight, "narrow"))
    mixed = residual.astype(jnp.float32) + sum(share.astype(jnp.float32) for share in shares)
    return (mixed.astype(jnp.bfloat16), new_state)


def solution(mesh):
    placed = (
        P(None, "kv"),
        P("kv"),
        P("kv", "tp"),
        P("kv", "tp"),
        P("kv", "tp"),
        P("kv", "tp"),
        P(),
        P(),
        P("tp"),
        P(),
        P("kv", "tp", None, None),
        P("kv", "tp", None, None),
        P("kv", "tp", None, None),
        P("kv", "tp", None),
        P("kv", "tp", None),
        P("kv"),
        P("tp", "kv"),
        P(),
        P("kv", "tp"),
        P("tp", "kv"),
    )
    return jax.shard_map(
        body,
        mesh=mesh,
        in_specs=placed,
        out_specs=(P(None, "kv"), P("kv", "tp", None, None)),
        check_vma=False,
    )
```

```python
import functools

import jax
import jax.numpy as jnp
from jax import lax
from jax.experimental import pallas as pl
from jax.experimental.pallas import tpu as pltpu
from jax.sharding import PartitionSpec as P

MODEL = 2048
EPS = 1e-06
LANES = 128
MEASURED_ORDERS = {8: (5, 7, 1, 4, 6, 3, 0, 2)}
VMEM = pltpu.VMEM
SMEM = pltpu.SMEM


def in_vmem():
    return pl.BlockSpec(memory_space=VMEM)


def room(megabytes):
    return pltpu.CompilerParams(vmem_limit_bytes=megabytes << 20)


def held(value):
    return pltpu.with_memory_space_constraint(value, VMEM)


def afar(value):
    return pltpu.with_memory_space_constraint(value, pltpu.HBM)


def in_smem():
    return pl.BlockSpec(memory_space=SMEM)


def dot(left, right, contract=((1,), (0,)), precision=None):
    return lax.dot_general(
        left,
        right,
        (contract, ((), ())),
        precision=precision,
        preferred_element_type=jnp.float32,
    )


def halves(value):
    high = value.astype(jnp.bfloat16).astype(jnp.float32)
    return high, value - high


def exchange_order(parts):
    if parts in MEASURED_ORDERS:
        return list(MEASURED_ORDERS[parts])
    stride = 3 if parts % 3 else 1
    return [(parts // 2 + 1 + stride * i) % parts for i in range(parts)]


def deal(out_ref, lanes, value):
    parts, rows, _ = out_ref.shape
    for slot, place in enumerate(exchange_order(parts)):
        out_ref[slot, :, lanes] = value[place * rows : (place + 1) * rows].astype(jnp.bfloat16)


def project_kernel(
    tokens_ref,
    gain_ref,
    beta_ref,
    decay_ref,
    mlp_gain_ref,
    *rest,
    count,
    extras,
    sliced,
):
    far, rest = rest[:count], rest[count:]
    far_extras, rest = rest[:extras], rest[extras:]
    (out_ref, near_tokens_ref, near_mlp_gain_ref), rest = rest[:3], rest[3:]
    near_extras, rest = rest[:extras], rest[extras:]
    (gain_row, beta_rows, decay_rows), rest = rest[:3], rest[3:]
    near, semaphore = rest[:count], rest[count]
    columns = tokens_ref.shape[1]
    part = pl.ds(0 if sliced else lax.axis_index("kv") * columns, columns)
    pairs = [
        (tokens_ref, near_tokens_ref),
        (gain_ref, gain_row),
        (beta_ref.at[:, part], beta_rows),
        (decay_ref.at[:, part], decay_rows),
    ]
    pairs += list(zip(far, near)) + list(zip(far_extras, near_extras))
    pairs.append((mlp_gain_ref.at[:, part], near_mlp_gain_ref))
    copies = [
        pltpu.make_async_copy(source, target, semaphore.at[i])
        for i, (source, target) in enumerate(pairs)
    ]
    for copy in copies:
        copy.start()
    for copy in copies[:4]:
        copy.wait()
    tokens = near_tokens_ref[...].astype(jnp.float32)
    batch = tokens.shape[0]
    normed = (tokens * gain_row[...]).astype(jnp.bfloat16)
    squares = jnp.sum(tokens * tokens, axis=1, keepdims=True)
    heads = beta_rows.shape[0]
    small = jnp.concatenate(
        [
            beta_rows[...],
            decay_rows[...],
            jnp.zeros((LANES - 2 * heads, columns), jnp.bfloat16),
        ],
        axis=0,
    )
    gating = dot(normed, small, ((1,), (1,)))
    lane = lax.broadcasted_iota(jnp.int32, (batch, LANES), 1)
    high, low = halves(gating)
    square_high, square_low = halves(squares)
    tile = high + pltpu.roll(low, 2 * heads, axis=1)
    tile = jnp.where(lane == 4 * heads, square_high, tile)
    tile = jnp.where(lane == 4 * heads + 1, square_low, tile)
    width = near[0].shape[1]
    deal(out_ref, slice(count * width, count * width + LANES), tile)
    for i in range(count):
        copies[4 + i].wait()
        deal(out_ref, slice(i * width, (i + 1) * width), dot(normed, near[i][...]))
    for copy in copies[4 + count :]:
        copy.wait()


def project(parts, tokens, norm_gain, weights, beta_weight, decay_weight, mlp_gain, extras):
    batch, columns = tokens.shape
    width = weights[0].shape[1]
    count = len(weights)
    by_feature = [beta_weight.T, decay_weight.T, mlp_gain.reshape(1, -1)]
    heads = beta_weight.shape[1]
    sliced = bool(columns % LANES)
    if sliced:
        start = lax.axis_index("kv") * columns
        by_feature = [lax.dynamic_slice_in_dim(w, start, columns, 1) for w in by_feature]
    return pl.pallas_call(
        functools.partial(project_kernel, count=count, extras=len(extras), sliced=sliced),
        in_specs=[pl.BlockSpec(memory_space=pl.ANY)] * (5 + count + len(extras)),
        out_specs=[in_vmem()] * (3 + len(extras)),
        out_shape=[
            VMEM((parts, batch // parts, count * width + LANES), jnp.bfloat16),
            VMEM((batch, columns), jnp.bfloat16),
            VMEM((1, columns), jnp.float32),
        ]
        + [VMEM(extra.shape, extra.dtype) for extra in extras],
        scratch_shapes=[
            VMEM((1, columns), jnp.float32),
            VMEM((heads, columns), jnp.bfloat16),
            VMEM((heads, columns), jnp.bfloat16),
        ]
        + [VMEM((columns, width), jnp.bfloat16)] * count
        + [pltpu.SemaphoreType.DMA((5 + count + len(extras),))],
        compiler_params=room(4),
        name="project",
    )(
        afar(tokens),
        afar(norm_gain.reshape(1, columns)),
        *[afar(value) for value in by_feature + list(weights) + list(extras)],
    )


def block_kernel(
    live_ref,
    keys_ref,
    values_ref,
    betas_ref,
    decays_ref,
    far_state_ref,
    out_ref,
    state_ref,
    semaphore,
    *,
    heads,
    pack,
):
    pairs, slots, width = keys_ref.shape
    fetch = pltpu.make_async_copy(far_state_ref, state_ref, semaphore)
    fetch.start()
    owner_row = lax.broadcasted_iota(jnp.int32, (pairs, slots), 0) // heads
    limit = jnp.zeros((pairs, slots), jnp.int32)
    for s in range(pairs // heads):
        limit = jnp.where(owner_row == s, live_ref[:, s : s + 1] - 1, limit)
    pending = lax.broadcasted_iota(jnp.int32, (pairs, slots), 1) < limit
    betas = jnp.where(pending, betas_ref[...], 0.0)
    decays = jnp.where(pending, decays_ref[...], 0.0)
    upto = (
        lax.broadcasted_iota(jnp.int32, (slots, slots), 0)
        <= lax.broadcasted_iota(jnp.int32, (slots, slots), 1)
    ).astype(jnp.float32)
    totals = dot(decays, upto, precision=lax.Precision.HIGHEST)
    columns = jnp.concatenate([totals, betas], axis=0).T
    total_columns = columns[:, :pairs]
    beta_columns = columns[:, pairs:]
    ending = total_columns[slots - 1 : slots, :]
    grown = jnp.exp(total_columns)
    faded = jnp.exp(ending - total_columns)
    whole_fade = jnp.exp(totals[:, slots - 1 : slots])
    across = pack * slots
    row = lax.broadcasted_iota(jnp.int32, (slots, across), 0)
    lane = lax.broadcasted_iota(jnp.int32, (slots, across), 1)
    column = lane % slots
    owner = lane // slots
    strict = row > column
    identity = (row == column).astype(jnp.float32)
    sizes = []
    size = 1
    while size < slots:
        sizes.append(size)
        size *= 2
    joins = [(row // (2 * s) == column // (2 * s)) & (row // s != column // s) for s in sizes]

    def choose(pieces):
        chosen = pieces[-1]
        for m in range(pack - 2, -1, -1):
            chosen = jnp.where(owner == m, pieces[m], chosen)
        return chosen

    def spread_out(value):
        return jnp.concatenate(
            [jnp.where(owner == m, value, 0.0).astype(jnp.bfloat16) for m in range(pack)], axis=0
        )

    packs = range(pairs // pack)
    lower = []
    inverse = []
    for g in packs:
        members = range(g * pack, (g + 1) * pack)
        stacked = keys_ref[g * pack : (g + 1) * pack].reshape(across, width)
        overlaps = dot(stacked, stacked, ((1,), (1,)))
        overlap = choose([overlaps[m * slots : (m + 1) * slots] for m in range(pack)])
        along = jnp.concatenate([totals[p : p + 1, :] for p in members], axis=1)
        down = choose([total_columns[:, p : p + 1] for p in members])
        beta = choose([beta_columns[:, p : p + 1] for p in members])
        weight = jnp.exp(jnp.where(strict, down - along, 0.0))
        lower.append(jnp.where(strict, beta * overlap * weight, 0.0))
        inverse.append(identity - jnp.where(joins[0], lower[g], 0.0))
    for level in range(1, len(sizes)):
        middle = [
            dot(
                inverse[g].astype(jnp.bfloat16),
                spread_out(jnp.where(joins[level], lower[g], 0.0)),
            )
            for g in packs
        ]
        for g in packs:
            inverse[g] = inverse[g] - dot(middle[g].astype(jnp.bfloat16), spread_out(inverse[g]))
    fetch.wait()
    for g in packs:
        members = range(g * pack, (g + 1) * pack)
        wanted = []
        for p in members:
            recalled = dot(keys_ref[p], state_ref[p].astype(jnp.bfloat16))
            wanted.append(
                beta_columns[:, p : p + 1]
                * (values_ref[p].astype(jnp.float32) - grown[:, p : p + 1] * recalled)
            )
        wanted = jnp.concatenate(wanted, axis=0).astype(jnp.bfloat16)
        updates = dot(spread_out(inverse[g]), wanted)
        for m, p in enumerate(members):
            update = faded[:, p : p + 1] * updates[m * slots : (m + 1) * slots]
            made = dot(keys_ref[p], update.astype(jnp.bfloat16), ((0,), (0,)))
            out_ref[p] = whole_fade[p : p + 1, :] * state_ref[p] + made


def block_state(live_count, keys, values, betas, decays, state, pack=4):
    seqs, heads, slots, width = keys.shape
    pairs = seqs * heads
    return pl.pallas_call(
        functools.partial(block_kernel, heads=heads, pack=pack),
        in_specs=[in_vmem()] * 5 + [pl.BlockSpec(memory_space=pl.ANY)],
        out_specs=in_vmem(),
        scratch_shapes=[VMEM((pairs, width, width), jnp.float32), pltpu.SemaphoreType.DMA],
        out_shape=VMEM((pairs, width, width), jnp.float32),
        cost_estimate=pl.CostEstimate(
            flops=60_000_000, bytes_accessed=5_000_000, transcendentals=0
        ),
        compiler_params=room(24),
        name="block_state",
    )(
        held(live_count),
        held(keys.reshape(pairs, slots, width)),
        held(values.reshape(pairs, slots, width)),
        held(betas),
        held(decays),
        afar(state.reshape(pairs, width, width)),
    )


def newest_kernel(
    rate_ref,
    arrived_ref,
    state_ref,
    gain_ref,
    mixed_ref,
    update_ref,
    columns_ref,
    fade_ref,
    recalled_ref,
    answered_ref,
    *,
    heads,
    total_heads,
):
    seqs = arrived_ref.shape[1]
    width = state_ref.shape[1]
    summed = jnp.sum(arrived_ref[...].astype(jnp.float32), axis=0)
    raw = lambda i, h: summed[:, (i * heads + h) * width : (i * heads + h + 1) * width]
    key_and_query = [raw(1, h) for h in range(heads)] + [raw(0, h) for h in range(heads)]
    columns = jnp.concatenate(key_and_query, axis=0).T
    columns_ref[...] = columns
    lines = [
        jnp.concatenate([raw(1, h), raw(0, h)], axis=0).astype(jnp.bfloat16) for h in range(heads)
    ]
    for h in range(heads):
        for s in range(seqs):
            found = dot(lines[h], state_ref[s * heads + h].astype(jnp.bfloat16))
            j = h * seqs + s
            recalled_ref[j : j + 1, :] = found[s : s + 1, :]
            answered_ref[j : j + 1, :] = found[seqs + s : seqs + s + 1, :]
    tail = summed[:, 4 * heads * width :]
    lane = lax.broadcasted_iota(jnp.int32, (seqs, LANES), 1)
    is_square = (lane == 4 * total_heads) | (lane == 4 * total_heads + 1)
    squares = jnp.sum(jnp.where(is_square, tail, 0.0), axis=1, keepdims=True)
    scale = lax.rsqrt(squares / MODEL + EPS)
    gating = (tail + pltpu.roll(tail, LANES - 2 * total_heads, axis=1)) * scale
    first = lax.axis_index("tp") * heads
    pick = lambda at: jnp.sum(jnp.where(lane == at, gating, 0.0), axis=1, keepdims=True)
    for h in range(heads):
        beta = jax.nn.sigmoid(pick(first + h))
        before = pick(total_heads + first + h)
        softplus = jnp.maximum(before, 0.0) + jnp.log1p(jnp.exp(-jnp.abs(before)))
        fade = jnp.exp(-rate_ref[:, h : h + 1] * softplus)
        rows = slice(h * seqs, (h + 1) * seqs)
        key = raw(1, h) * scale
        key_scale = lax.rsqrt(jnp.sum(key * key, axis=1, keepdims=True) + EPS)
        query = raw(0, h) * scale
        agreement = jnp.sum(key * query, axis=1, keepdims=True) * key_scale
        value = raw(2, h) * scale
        gate = raw(3, h) * scale
        update = beta * (value - fade * (key_scale * scale) * recalled_ref[rows, :])
        readout = fade * scale * answered_ref[rows, :] + agreement * update
        power = jnp.mean(readout * readout, axis=1, keepdims=True)
        mixed = readout * lax.rsqrt(power + EPS) * gain_ref[...] * (gate * jax.nn.sigmoid(gate))
        shape = (mixed_ref.shape[0], seqs, width)
        mixed_ref[:, :, h * width : (h + 1) * width] = jnp.broadcast_to(mixed[None], shape).astype(
            jnp.bfloat16
        )
        update_ref[rows, :] = update * (key_scale * scale)
        fade_ref[rows, :] = jnp.broadcast_to(fade, (seqs, width))


def newest(decay_rate, arrived, state, head_gain, heads, total_heads):
    parts, seqs, _ = arrived.shape
    width = state.shape[1]
    count = heads * seqs
    return pl.pallas_call(
        functools.partial(newest_kernel, heads=heads, total_heads=total_heads),
        in_specs=[in_vmem()] * 4,
        out_specs=[in_vmem()] * 4,
        out_shape=[
            VMEM((parts, seqs, heads * width), jnp.bfloat16),
            VMEM((count, width), jnp.float32),
            VMEM((width, 2 * count), jnp.float32),
            VMEM((count, width), jnp.float32),
        ],
        scratch_shapes=[pltpu.VMEM((count, width), jnp.float32)] * 2,
        compiler_params=room(4),
        name="newest",
    )(
        held(decay_rate),
        held(arrived),
        held(state),
        held(head_gain),
    )


def refresh_kernel(state_ref, update_ref, columns_ref, fade_ref, out_ref, made_ref, semaphore):
    pairs = state_ref.shape[0]
    seqs = made_ref.shape[0]
    heads = pairs // seqs
    columns = columns_ref[...]
    copies = []
    for s in range(seqs):
        for h in range(heads):
            j = h * seqs + s
            made_ref[s, h] = (
                fade_ref[j : j + 1, :] * state_ref[s * heads + h]
                + columns[:, j : j + 1] * update_ref[j : j + 1, :]
            )
        copies.append(pltpu.make_async_copy(made_ref.at[s], out_ref.at[s], semaphore.at[s]))
        copies[-1].start()
    for copy in copies:
        copy.wait()


def refresh(state, update, columns, fade, seqs):
    pairs, width, _ = state.shape
    shape = (seqs, pairs // seqs, width, width)
    return pl.pallas_call(
        refresh_kernel,
        in_specs=[in_vmem()] * 4,
        out_specs=pl.BlockSpec(memory_space=pl.ANY),
        out_shape=jax.ShapeDtypeStruct(shape, jnp.float32),
        scratch_shapes=[pltpu.VMEM(shape, jnp.float32), pltpu.SemaphoreType.DMA((seqs,))],
        cost_estimate=pl.CostEstimate(
            flops=10_000_000, bytes_accessed=4_000_000, transcendentals=0
        ),
        compiler_params=room(8),
        name="refresh",
    )(held(state), held(update), held(columns), held(fade))


def widen_kernel(residual_ref, scaled_ref, weight_ref, out_ref):
    value = residual_ref[...].astype(jnp.float32)
    batch = value.shape[0]
    high, low = halves(jnp.sum(value * value, axis=1, keepdims=True))
    lane = lax.broadcasted_iota(jnp.int32, (batch, LANES), 1)
    tile = jnp.where(lane == 0, high, jnp.where(lane == 1, low, 0.0))
    units = weight_ref.shape[1]
    deal(out_ref, slice(units, units + LANES), tile)
    deal(out_ref, slice(0, units), dot(scaled_ref[...], weight_ref[...]))


def widen(parts, residual, scaled, up_weight):
    batch = residual.shape[0]
    units = up_weight.shape[1]
    return pl.pallas_call(
        widen_kernel,
        in_specs=[in_vmem()] * 3,
        out_specs=in_vmem(),
        out_shape=VMEM((parts, batch // parts, units + LANES), jnp.bfloat16),
        compiler_params=room(6),
        name="widen",
    )(held(residual), held(scaled), held(up_weight))


def activate_kernel(arrived_ref, out_ref):
    units = out_ref.shape[2]
    summed = jnp.sum(arrived_ref[...].astype(jnp.float32), axis=0)
    tail = summed[:, units:]
    lane = lax.broadcasted_iota(jnp.int32, tail.shape, 1)
    squares = jnp.sum(jnp.where(lane < 2, tail, 0.0), axis=1, keepdims=True)
    scale = lax.rsqrt(squares / MODEL + EPS)
    hidden = jnp.square(jnp.maximum(summed[:, :units] * scale, 0.0))
    out_ref[...] = jnp.broadcast_to(hidden[None], out_ref.shape).astype(jnp.bfloat16)


def activate(arrived):
    parts, seqs, wide = arrived.shape
    return pl.pallas_call(
        activate_kernel,
        in_specs=[in_vmem()],
        out_specs=in_vmem(),
        out_shape=VMEM((parts, seqs, wide - LANES), jnp.bfloat16),
        compiler_params=room(4),
        name="activate",
    )(held(arrived))


def narrow_kernel(rows_ref, weight_ref, out_ref):
    parts, rows, width = rows_ref.shape
    made = dot(rows_ref[...].reshape(parts * rows, width), weight_ref[...])
    order = exchange_order(parts)
    slots = [order.index(place) for place in range(parts)]
    pieces = [made[slot * rows : (slot + 1) * rows] for slot in slots]
    out_ref[...] = jnp.concatenate(pieces, axis=0).astype(jnp.bfloat16)


def narrow(rows, weight, name):
    return pl.pallas_call(
        narrow_kernel,
        in_specs=[in_vmem()] * 2,
        out_specs=in_vmem(),
        out_shape=VMEM((rows.shape[0] * rows.shape[1], weight.shape[1]), jnp.bfloat16),
        compiler_params=room(4),
        name=name,
    )(held(rows), held(weight))


def swap_over_kv(payload):
    groups = [exchange_order(payload.shape[0])]
    return lax.all_to_all(payload, "kv", 0, 0, axis_index_groups=groups, tiled=True)


def over_tp(mine):
    count = lax.axis_size("tp")
    parts = [mine]
    for step in range(1, count):
        swaps = [(place, place ^ step) for place in range(count)]
        parts.append(lax.ppermute(mine, "tp", swaps))
    return parts


def body(
    tokens,
    norm_gain,
    query_weight,
    key_weight,
    value_weight,
    gate_weight,
    beta_weight,
    decay_weight,
    decay_rate,
    head_gain,
    carried_state,
    block_keys,
    block_values,
    block_beta,
    block_decay,
    live_count,
    out_weight,
    mlp_gain,
    up_weight,
    down_weight,
):
    parts = lax.axis_size("kv")
    seqs, heads, slots, width = block_keys.shape
    pairs = seqs * heads
    payload, near_tokens, gain, live, betas, decays, rates, head_gains = project(
        parts,
        tokens,
        norm_gain,
        [query_weight, key_weight, value_weight, gate_weight],
        beta_weight,
        decay_weight,
        mlp_gain,
        [
            live_count.reshape(1, seqs),
            block_beta.reshape(pairs, slots),
            block_decay.reshape(pairs, slots),
            decay_rate.reshape(1, heads),
            head_gain.reshape(1, width),
        ],
    )
    arrived = swap_over_kv(payload)
    state = block_state(live, block_keys, block_values, betas, decays, carried_state)
    copies, update, columns, fade = newest(
        rates, arrived, state, head_gains, heads, beta_weight.shape[1]
    )
    new_state = refresh(state, update, columns, fade, seqs)
    attended = over_tp(narrow(swap_over_kv(copies), out_weight, "attend"))
    residual = near_tokens.astype(jnp.float32) + sum(part.astype(jnp.float32) for part in attended)
    residual = residual.astype(jnp.bfloat16)
    scaled = (residual.astype(jnp.float32) * gain).astype(jnp.bfloat16)
    hidden = activate(swap_over_kv(widen(parts, residual, scaled, up_weight)))
    shares = over_tp(narrow(swap_over_kv(hidden), down_weight, "narrow"))
    mixed = residual.astype(jnp.float32) + sum(share.astype(jnp.float32) for share in shares)
    return (mixed.astype(jnp.bfloat16), new_state)


def solution(mesh):
    placed = (
        P(None, "kv"),
        P("kv"),
        P("kv", "tp"),
        P("kv", "tp"),
        P("kv", "tp"),
        P("kv", "tp"),
        P(),
        P(),
        P("tp"),
        P(),
        P("kv", "tp", None, None),
        P("kv", "tp", None, None),
        P("kv", "tp", None, None),
        P("kv", "tp", None),
        P("kv", "tp", None),
        P("kv"),
        P("tp", "kv"),
        P(),
        P("kv", "tp"),
        P("tp", "kv"),
    )
    return jax.shard_map(
        body,
        mesh=mesh,
        in_specs=placed,
        out_specs=(P(None, "kv"), P("kv", "tp", None, None)),
        check_vma=False,
    )
```

```python
import functools

import jax
import jax.numpy as jnp
from jax import lax
from jax.experimental import pallas as pl
from jax.experimental.pallas import tpu as pltpu
from jax.sharding import PartitionSpec as P

MODEL = 2048
EPS = 1e-06
LANES = 128
MEASURED_ORDERS = {8: (5, 7, 1, 4, 6, 3, 0, 2)}
VMEM = pltpu.VMEM
SMEM = pltpu.SMEM


def in_vmem():
    return pl.BlockSpec(memory_space=VMEM)


def room(megabytes):
    return pltpu.CompilerParams(vmem_limit_bytes=megabytes << 20)


def held(value):
    return pltpu.with_memory_space_constraint(value, VMEM)


def afar(value):
    return pltpu.with_memory_space_constraint(value, pltpu.HBM)


def in_smem():
    return pl.BlockSpec(memory_space=SMEM)


def dot(left, right, contract=((1,), (0,)), precision=None):
    return lax.dot_general(
        left,
        right,
        (contract, ((), ())),
        precision=precision,
        preferred_element_type=jnp.float32,
    )


def halves(value):
    high = value.astype(jnp.bfloat16).astype(jnp.float32)
    return high, value - high


def exchange_order(parts):
    if parts in MEASURED_ORDERS:
        return list(MEASURED_ORDERS[parts])
    stride = 3 if parts % 3 else 1
    return [(parts // 2 + 1 + stride * i) % parts for i in range(parts)]


def deal(out_ref, lanes, value):
    parts, rows, _ = out_ref.shape
    for slot, place in enumerate(exchange_order(parts)):
        out_ref[slot, :, lanes] = value[place * rows : (place + 1) * rows].astype(jnp.bfloat16)


def project_kernel(
    tokens_ref,
    gain_ref,
    beta_ref,
    decay_ref,
    mlp_gain_ref,
    *rest,
    count,
    extras,
    sliced,
):
    far, rest = rest[:count], rest[count:]
    far_extras, rest = rest[:extras], rest[extras:]
    (far_out_ref, near_tokens_ref, near_mlp_gain_ref), rest = rest[:3], rest[3:]
    near_extras, rest = rest[:extras], rest[extras:]
    (out_ref, gain_row, beta_rows, decay_rows), rest = rest[:4], rest[4:]
    near, semaphore, leaving = rest[:count], rest[count], rest[count + 1]
    columns = tokens_ref.shape[1]
    part = pl.ds(0 if sliced else lax.axis_index("kv") * columns, columns)
    pairs = [
        (tokens_ref, near_tokens_ref),
        (gain_ref, gain_row),
        (beta_ref.at[:, part], beta_rows),
        (decay_ref.at[:, part], decay_rows),
    ]
    pairs += list(zip(far, near)) + list(zip(far_extras, near_extras))
    pairs.append((mlp_gain_ref.at[:, part], near_mlp_gain_ref))
    copies = [
        pltpu.make_async_copy(source, target, semaphore.at[i])
        for i, (source, target) in enumerate(pairs)
    ]
    for copy in copies:
        copy.start()
    for copy in copies[:4]:
        copy.wait()
    tokens = near_tokens_ref[...].astype(jnp.float32)
    batch = tokens.shape[0]
    normed = (tokens * gain_row[...]).astype(jnp.bfloat16)
    squares = jnp.sum(tokens * tokens, axis=1, keepdims=True)
    heads = beta_rows.shape[0]
    small = jnp.concatenate(
        [
            beta_rows[...],
            decay_rows[...],
            jnp.zeros((LANES - 2 * heads, columns), jnp.bfloat16),
        ],
        axis=0,
    )
    gating = dot(normed, small, ((1,), (1,)))
    lane = lax.broadcasted_iota(jnp.int32, (batch, LANES), 1)
    high, low = halves(gating)
    square_high, square_low = halves(squares)
    tile = high + pltpu.roll(low, 2 * heads, axis=1)
    tile = jnp.where(lane == 4 * heads, square_high, tile)
    tile = jnp.where(lane == 4 * heads + 1, square_low, tile)
    width = near[0].shape[1]
    departures = []

    def depart(lanes, value):
        deal(out_ref, lanes, value)
        source, target = out_ref.at[:, :, lanes], far_out_ref.at[:, :, lanes]
        semaphore_here = leaving.at[len(departures)]
        departures.append(pltpu.make_async_copy(source, target, semaphore_here))
        departures[-1].start()

    depart(slice(count * width, count * width + LANES), tile)
    for i in range(count):
        copies[4 + i].wait()
        depart(slice(i * width, (i + 1) * width), dot(normed, near[i][...]))
    for copy in copies[4 + count :] + departures:
        copy.wait()


def project(parts, tokens, norm_gain, weights, beta_weight, decay_weight, mlp_gain, extras):
    batch, columns = tokens.shape
    width = weights[0].shape[1]
    count = len(weights)
    by_feature = [beta_weight.T, decay_weight.T, mlp_gain.reshape(1, -1)]
    heads = beta_weight.shape[1]
    sliced = bool(columns % LANES)
    if sliced:
        start = lax.axis_index("kv") * columns
        by_feature = [lax.dynamic_slice_in_dim(w, start, columns, 1) for w in by_feature]
    return pl.pallas_call(
        functools.partial(project_kernel, count=count, extras=len(extras), sliced=sliced),
        in_specs=[pl.BlockSpec(memory_space=pl.ANY)] * (5 + count + len(extras)),
        out_specs=[pl.BlockSpec(memory_space=pl.ANY)] + [in_vmem()] * (2 + len(extras)),
        out_shape=[
            pltpu.HBM((parts, batch // parts, count * width + LANES), jnp.bfloat16),
            VMEM((batch, columns), jnp.bfloat16),
            VMEM((1, columns), jnp.float32),
        ]
        + [VMEM(extra.shape, extra.dtype) for extra in extras],
        scratch_shapes=[
            VMEM((parts, batch // parts, count * width + LANES), jnp.bfloat16),
            VMEM((1, columns), jnp.float32),
            VMEM((heads, columns), jnp.bfloat16),
            VMEM((heads, columns), jnp.bfloat16),
        ]
        + [VMEM((columns, width), jnp.bfloat16)] * count
        + [
            pltpu.SemaphoreType.DMA((5 + count + len(extras),)),
            pltpu.SemaphoreType.DMA((1 + count,)),
        ],
        compiler_params=room(4),
        name="project",
    )(
        afar(tokens),
        afar(norm_gain.reshape(1, columns)),
        *[afar(value) for value in by_feature + list(weights) + list(extras)],
    )


def block_kernel(
    live_ref,
    keys_ref,
    values_ref,
    betas_ref,
    decays_ref,
    far_state_ref,
    out_ref,
    state_ref,
    semaphore,
    *,
    heads,
    pack,
):
    pairs, slots, width = keys_ref.shape
    fetch = pltpu.make_async_copy(far_state_ref, state_ref, semaphore)
    fetch.start()
    owner_row = lax.broadcasted_iota(jnp.int32, (pairs, slots), 0) // heads
    limit = jnp.zeros((pairs, slots), jnp.int32)
    for s in range(pairs // heads):
        limit = jnp.where(owner_row == s, live_ref[:, s : s + 1] - 1, limit)
    pending = lax.broadcasted_iota(jnp.int32, (pairs, slots), 1) < limit
    betas = jnp.where(pending, betas_ref[...], 0.0)
    decays = jnp.where(pending, decays_ref[...], 0.0)
    upto = (
        lax.broadcasted_iota(jnp.int32, (slots, slots), 0)
        <= lax.broadcasted_iota(jnp.int32, (slots, slots), 1)
    ).astype(jnp.float32)
    totals = dot(decays, upto, precision=lax.Precision.HIGHEST)
    columns = jnp.concatenate([totals, betas], axis=0).T
    total_columns = columns[:, :pairs]
    beta_columns = columns[:, pairs:]
    ending = total_columns[slots - 1 : slots, :]
    grown = jnp.exp(total_columns)
    faded = jnp.exp(ending - total_columns)
    whole_fade = jnp.exp(totals[:, slots - 1 : slots])
    across = pack * slots
    row = lax.broadcasted_iota(jnp.int32, (slots, across), 0)
    lane = lax.broadcasted_iota(jnp.int32, (slots, across), 1)
    column = lane % slots
    owner = lane // slots
    strict = row > column
    identity = (row == column).astype(jnp.float32)
    sizes = []
    size = 1
    while size < slots:
        sizes.append(size)
        size *= 2
    joins = [(row // (2 * s) == column // (2 * s)) & (row // s != column // s) for s in sizes]

    def choose(pieces):
        chosen = pieces[-1]
        for m in range(pack - 2, -1, -1):
            chosen = jnp.where(owner == m, pieces[m], chosen)
        return chosen

    def spread_out(value):
        return jnp.concatenate(
            [jnp.where(owner == m, value, 0.0).astype(jnp.bfloat16) for m in range(pack)], axis=0
        )

    packs = range(pairs // pack)
    lower = []
    inverse = []
    for g in packs:
        members = range(g * pack, (g + 1) * pack)
        stacked = keys_ref[g * pack : (g + 1) * pack].reshape(across, width)
        overlaps = dot(stacked, stacked, ((1,), (1,)))
        overlap = choose([overlaps[m * slots : (m + 1) * slots] for m in range(pack)])
        along = jnp.concatenate([totals[p : p + 1, :] for p in members], axis=1)
        down = choose([total_columns[:, p : p + 1] for p in members])
        beta = choose([beta_columns[:, p : p + 1] for p in members])
        weight = jnp.exp(jnp.where(strict, down - along, 0.0))
        lower.append(jnp.where(strict, beta * overlap * weight, 0.0))
        inverse.append(identity - jnp.where(joins[0], lower[g], 0.0))
    for level in range(1, len(sizes)):
        middle = [
            dot(
                inverse[g].astype(jnp.bfloat16),
                spread_out(jnp.where(joins[level], lower[g], 0.0)),
            )
            for g in packs
        ]
        for g in packs:
            inverse[g] = inverse[g] - dot(middle[g].astype(jnp.bfloat16), spread_out(inverse[g]))
    fetch.wait()
    for g in packs:
        members = range(g * pack, (g + 1) * pack)
        wanted = []
        for p in members:
            recalled = dot(keys_ref[p], state_ref[p].astype(jnp.bfloat16))
            wanted.append(
                beta_columns[:, p : p + 1]
                * (values_ref[p].astype(jnp.float32) - grown[:, p : p + 1] * recalled)
            )
        wanted = jnp.concatenate(wanted, axis=0).astype(jnp.bfloat16)
        updates = dot(spread_out(inverse[g]), wanted)
        for m, p in enumerate(members):
            update = faded[:, p : p + 1] * updates[m * slots : (m + 1) * slots]
            made = dot(keys_ref[p], update.astype(jnp.bfloat16), ((0,), (0,)))
            out_ref[p] = whole_fade[p : p + 1, :] * state_ref[p] + made


def block_state(live_count, keys, values, betas, decays, state, pack=4):
    seqs, heads, slots, width = keys.shape
    pairs = seqs * heads
    return pl.pallas_call(
        functools.partial(block_kernel, heads=heads, pack=pack),
        in_specs=[in_vmem()] * 5 + [pl.BlockSpec(memory_space=pl.ANY)],
        out_specs=in_vmem(),
        scratch_shapes=[VMEM((pairs, width, width), jnp.float32), pltpu.SemaphoreType.DMA],
        out_shape=VMEM((pairs, width, width), jnp.float32),
        cost_estimate=pl.CostEstimate(
            flops=60_000_000, bytes_accessed=5_000_000, transcendentals=0
        ),
        compiler_params=room(24),
        name="block_state",
    )(
        held(live_count),
        held(keys.reshape(pairs, slots, width)),
        held(values.reshape(pairs, slots, width)),
        held(betas),
        held(decays),
        afar(state.reshape(pairs, width, width)),
    )


def newest_kernel(
    rate_ref,
    arrived_ref,
    state_ref,
    gain_ref,
    mixed_ref,
    update_ref,
    columns_ref,
    fade_ref,
    recalled_ref,
    answered_ref,
    *,
    heads,
    total_heads,
):
    seqs = arrived_ref.shape[1]
    width = state_ref.shape[1]
    summed = jnp.sum(arrived_ref[...].astype(jnp.float32), axis=0)
    raw = lambda i, h: summed[:, (i * heads + h) * width : (i * heads + h + 1) * width]
    key_and_query = [raw(1, h) for h in range(heads)] + [raw(0, h) for h in range(heads)]
    columns = jnp.concatenate(key_and_query, axis=0).T
    columns_ref[...] = columns
    lines = [
        jnp.concatenate([raw(1, h), raw(0, h)], axis=0).astype(jnp.bfloat16) for h in range(heads)
    ]
    for h in range(heads):
        for s in range(seqs):
            found = dot(lines[h], state_ref[s * heads + h].astype(jnp.bfloat16))
            j = h * seqs + s
            recalled_ref[j : j + 1, :] = found[s : s + 1, :]
            answered_ref[j : j + 1, :] = found[seqs + s : seqs + s + 1, :]
    tail = summed[:, 4 * heads * width :]
    lane = lax.broadcasted_iota(jnp.int32, (seqs, LANES), 1)
    is_square = (lane == 4 * total_heads) | (lane == 4 * total_heads + 1)
    squares = jnp.sum(jnp.where(is_square, tail, 0.0), axis=1, keepdims=True)
    scale = lax.rsqrt(squares / MODEL + EPS)
    gating = (tail + pltpu.roll(tail, LANES - 2 * total_heads, axis=1)) * scale
    first = lax.axis_index("tp") * heads
    pick = lambda at: jnp.sum(jnp.where(lane == at, gating, 0.0), axis=1, keepdims=True)
    for h in range(heads):
        beta = jax.nn.sigmoid(pick(first + h))
        before = pick(total_heads + first + h)
        softplus = jnp.maximum(before, 0.0) + jnp.log1p(jnp.exp(-jnp.abs(before)))
        fade = jnp.exp(-rate_ref[:, h : h + 1] * softplus)
        rows = slice(h * seqs, (h + 1) * seqs)
        key = raw(1, h) * scale
        key_scale = lax.rsqrt(jnp.sum(key * key, axis=1, keepdims=True) + EPS)
        query = raw(0, h) * scale
        agreement = jnp.sum(key * query, axis=1, keepdims=True) * key_scale
        value = raw(2, h) * scale
        gate = raw(3, h) * scale
        update = beta * (value - fade * (key_scale * scale) * recalled_ref[rows, :])
        readout = fade * scale * answered_ref[rows, :] + agreement * update
        power = jnp.mean(readout * readout, axis=1, keepdims=True)
        mixed = readout * lax.rsqrt(power + EPS) * gain_ref[...] * (gate * jax.nn.sigmoid(gate))
        shape = (mixed_ref.shape[0], seqs, width)
        mixed_ref[:, :, h * width : (h + 1) * width] = jnp.broadcast_to(mixed[None], shape).astype(
            jnp.bfloat16
        )
        update_ref[rows, :] = update * (key_scale * scale)
        fade_ref[rows, :] = jnp.broadcast_to(fade, (seqs, width))


def newest(decay_rate, arrived, state, head_gain, heads, total_heads):
    parts, seqs, _ = arrived.shape
    width = state.shape[1]
    count = heads * seqs
    return pl.pallas_call(
        functools.partial(newest_kernel, heads=heads, total_heads=total_heads),
        in_specs=[in_vmem()] * 4,
        out_specs=[in_vmem()] * 4,
        out_shape=[
            VMEM((parts, seqs, heads * width), jnp.bfloat16),
            VMEM((count, width), jnp.float32),
            VMEM((width, 2 * count), jnp.float32),
            VMEM((count, width), jnp.float32),
        ],
        scratch_shapes=[pltpu.VMEM((count, width), jnp.float32)] * 2,
        compiler_params=room(4),
        name="newest",
    )(
        held(decay_rate),
        held(arrived),
        held(state),
        held(head_gain),
    )


def refresh_kernel(state_ref, update_ref, columns_ref, fade_ref, out_ref, made_ref, semaphore):
    pairs = state_ref.shape[0]
    seqs = made_ref.shape[0]
    heads = pairs // seqs
    columns = columns_ref[...]
    copies = []
    for s in range(seqs):
        for h in range(heads):
            j = h * seqs + s
            made_ref[s, h] = (
                fade_ref[j : j + 1, :] * state_ref[s * heads + h]
                + columns[:, j : j + 1] * update_ref[j : j + 1, :]
            )
        copies.append(pltpu.make_async_copy(made_ref.at[s], out_ref.at[s], semaphore.at[s]))
        copies[-1].start()
    for copy in copies:
        copy.wait()


def refresh(state, update, columns, fade, seqs):
    pairs, width, _ = state.shape
    shape = (seqs, pairs // seqs, width, width)
    return pl.pallas_call(
        refresh_kernel,
        in_specs=[in_vmem()] * 4,
        out_specs=pl.BlockSpec(memory_space=pl.ANY),
        out_shape=jax.ShapeDtypeStruct(shape, jnp.float32),
        scratch_shapes=[pltpu.VMEM(shape, jnp.float32), pltpu.SemaphoreType.DMA((seqs,))],
        cost_estimate=pl.CostEstimate(
            flops=10_000_000, bytes_accessed=4_000_000, transcendentals=0
        ),
        compiler_params=room(8),
        name="refresh",
    )(held(state), held(update), held(columns), held(fade))


def widen_kernel(residual_ref, scaled_ref, weight_ref, out_ref):
    value = residual_ref[...].astype(jnp.float32)
    batch = value.shape[0]
    high, low = halves(jnp.sum(value * value, axis=1, keepdims=True))
    lane = lax.broadcasted_iota(jnp.int32, (batch, LANES), 1)
    tile = jnp.where(lane == 0, high, jnp.where(lane == 1, low, 0.0))
    units = weight_ref.shape[1]
    deal(out_ref, slice(units, units + LANES), tile)
    deal(out_ref, slice(0, units), dot(scaled_ref[...], weight_ref[...]))


def widen(parts, residual, scaled, up_weight):
    batch = residual.shape[0]
    units = up_weight.shape[1]
    return pl.pallas_call(
        widen_kernel,
        in_specs=[in_vmem()] * 3,
        out_specs=in_vmem(),
        out_shape=VMEM((parts, batch // parts, units + LANES), jnp.bfloat16),
        compiler_params=room(6),
        name="widen",
    )(held(residual), held(scaled), held(up_weight))


def activate_kernel(arrived_ref, out_ref):
    units = out_ref.shape[2]
    summed = jnp.sum(arrived_ref[...].astype(jnp.float32), axis=0)
    tail = summed[:, units:]
    lane = lax.broadcasted_iota(jnp.int32, tail.shape, 1)
    squares = jnp.sum(jnp.where(lane < 2, tail, 0.0), axis=1, keepdims=True)
    scale = lax.rsqrt(squares / MODEL + EPS)
    hidden = jnp.square(jnp.maximum(summed[:, :units] * scale, 0.0))
    out_ref[...] = jnp.broadcast_to(hidden[None], out_ref.shape).astype(jnp.bfloat16)


def activate(arrived):
    parts, seqs, wide = arrived.shape
    return pl.pallas_call(
        activate_kernel,
        in_specs=[in_vmem()],
        out_specs=in_vmem(),
        out_shape=VMEM((parts, seqs, wide - LANES), jnp.bfloat16),
        compiler_params=room(4),
        name="activate",
    )(held(arrived))


def narrow_kernel(rows_ref, weight_ref, out_ref):
    parts, rows, width = rows_ref.shape
    made = dot(rows_ref[...].reshape(parts * rows, width), weight_ref[...])
    order = exchange_order(parts)
    slots = [order.index(place) for place in range(parts)]
    pieces = [made[slot * rows : (slot + 1) * rows] for slot in slots]
    out_ref[...] = jnp.concatenate(pieces, axis=0).astype(jnp.bfloat16)


def narrow(rows, weight, name):
    return pl.pallas_call(
        narrow_kernel,
        in_specs=[in_vmem()] * 2,
        out_specs=in_vmem(),
        out_shape=VMEM((rows.shape[0] * rows.shape[1], weight.shape[1]), jnp.bfloat16),
        compiler_params=room(4),
        name=name,
    )(held(rows), held(weight))


def swap_over_kv(payload):
    groups = [exchange_order(payload.shape[0])]
    return lax.all_to_all(payload, "kv", 0, 0, axis_index_groups=groups, tiled=True)


def over_tp(mine):
    count = lax.axis_size("tp")
    parts = [mine]
    for step in range(1, count):
        swaps = [(place, place ^ step) for place in range(count)]
        parts.append(lax.ppermute(mine, "tp", swaps))
    return parts


def body(
    tokens,
    norm_gain,
    query_weight,
    key_weight,
    value_weight,
    gate_weight,
    beta_weight,
    decay_weight,
    decay_rate,
    head_gain,
    carried_state,
    block_keys,
    block_values,
    block_beta,
    block_decay,
    live_count,
    out_weight,
    mlp_gain,
    up_weight,
    down_weight,
):
    parts = lax.axis_size("kv")
    seqs, heads, slots, width = block_keys.shape
    pairs = seqs * heads
    payload, near_tokens, gain, live, betas, decays, rates, head_gains = project(
        parts,
        tokens,
        norm_gain,
        [query_weight, key_weight, value_weight, gate_weight],
        beta_weight,
        decay_weight,
        mlp_gain,
        [
            live_count.reshape(1, seqs),
            block_beta.reshape(pairs, slots),
            block_decay.reshape(pairs, slots),
            decay_rate.reshape(1, heads),
            head_gain.reshape(1, width),
        ],
    )
    arrived = swap_over_kv(payload)
    state = block_state(live, block_keys, block_values, betas, decays, carried_state)
    copies, update, columns, fade = newest(
        rates, arrived, state, head_gains, heads, beta_weight.shape[1]
    )
    new_state = refresh(state, update, columns, fade, seqs)
    attended = over_tp(narrow(swap_over_kv(copies), out_weight, "attend"))
    residual = near_tokens.astype(jnp.float32) + sum(part.astype(jnp.float32) for part in attended)
    residual = residual.astype(jnp.bfloat16)
    scaled = (residual.astype(jnp.float32) * gain).astype(jnp.bfloat16)
    hidden = activate(swap_over_kv(widen(parts, residual, scaled, up_weight)))
    shares = over_tp(narrow(swap_over_kv(hidden), down_weight, "narrow"))
    mixed = residual.astype(jnp.float32) + sum(share.astype(jnp.float32) for share in shares)
    return (mixed.astype(jnp.bfloat16), new_state)


def solution(mesh):
    placed = (
        P(None, "kv"),
        P("kv"),
        P("kv", "tp"),
        P("kv", "tp"),
        P("kv", "tp"),
        P("kv", "tp"),
        P(),
        P(),
        P("tp"),
        P(),
        P("kv", "tp", None, None),
        P("kv", "tp", None, None),
        P("kv", "tp", None, None),
        P("kv", "tp", None),
        P("kv", "tp", None),
        P("kv"),
        P("tp", "kv"),
        P(),
        P("kv", "tp"),
        P("tp", "kv"),
    )
    return jax.shard_map(
        body,
        mesh=mesh,
        in_specs=placed,
        out_specs=(P(None, "kv"), P("kv", "tp", None, None)),
        check_vma=False,
    )
```
